1024 devices in a mesh: fs: 128 (over z, y), tp: 8 (over x, core).
Axes of the slice: x: 4, y: 8, z: 16, core: 2. Of those that a mesh axis runs over, the one named last changes fastest.
Arguments:
- hidden_in: bfloat16 [1024, 4096], P(None, 'tp'), may hold values from -6 to 6
- up_act: bfloat16 [1024, 12288], P('tp', 'fs'), may hold values from -6 to 6
- up_val: bfloat16 [1024, 12288], P('tp', 'fs'), may hold values from -6 to 6
- cotangent: bfloat16 [1024, 4096], P('tp'), may hold values from -6 to 6
- w_act: bfloat16 [4096, 12288], P('tp', 'fs'), may hold values from -0.09375 to 0.09375
- w_val: bfloat16 [4096, 12288], P('tp', 'fs'), may hold values from -0.09375 to 0.09375
- w_down: bfloat16 [12288, 4096], P('fs', 'tp'), may hold values from -0.0546875 to 0.0546875
- conv_act: bfloat16 [3, 12288], P(None, 'fs'), may hold values from -3 to 3
- conv_val: bfloat16 [3, 12288], P(None, 'fs'), may hold values from -3 to 3
- bias_act: bfloat16 [12288], P('fs'), may hold values from -3 to 3
- bias_val: bfloat16 [12288], P('fs'), may hold values from -3 to 3
Outputs:
- grad_input: bfloat16 [1024, 4096], P(('tp', 'fs'))
- grad_w_act: float32 [4096, 12288], P('tp', 'fs')
- grad_w_val: float32 [4096, 12288], P('tp', 'fs')
- grad_w_down: float32 [12288, 4096], P('fs', 'tp')
- grad_conv_act: float32 [3, 12288], P(None, 'fs')
- grad_conv_val: float32 [3, 12288], P(None, 'fs')
- grad_bias_act: float32 [12288], P('fs')
- grad_bias_val: float32 [12288], P('fs')
- rows_act: float32 [4096], P('tp')
- rows_val: float32 [4096], P('tp')
- rows_down: float32 [12288], P('fs')
- conv_rows: float32 [2, 3], replicated
The draws below stay inside these ranges and needn't reach their ends.
All inputs are finite; a program needn't handle non-finite values.
Results may differ from the reference program's by a relative error of at most 0.0057.
Values may be sent and summed in bfloat16 or wider, within the bound.
A program may use at most 32 MiB of HBM per device.

```python
import jax
import jax.numpy as jnp
from jax import lax

D = 4096
FF = 12288
KW = 3
TOKENS = 1024


def with_spikes(result, own_key, source, target, parts, factor):
    owner, partner = [(jnp.arange(result.shape[axis_at]) // (result.shape[axis_at] // parts)).reshape([-1 if axis == axis_at else 1 for axis in range(result.ndim)]) for axis_at in (source, target)]
    chosen = jax.random.permutation(own_key, parts)[partner]
    strong = (owner == chosen) | (owner == (partner + parts // 2) % parts)
    return jnp.where(strong, factor * result, result)


def shard_levels(own_key, shape, cuts, smallest, top_value):
    level = 1.0
    for axis_at, parts in cuts:
        draws = jax.random.uniform(jax.random.fold_in(jax.random.fold_in(own_key, 6), axis_at), (parts,), jnp.float32, smallest / len(cuts), top_value / len(cuts))
        level = level * jnp.repeat(jnp.exp(draws), shape[axis_at] // parts).reshape((-1,) + (1,) * (len(shape) - 1 - axis_at))
    return level


def bell_draw(own_key, extent, deviation, bound, pieces=(), held_as=jnp.bfloat16):
    values = deviation * jax.random.normal(own_key, extent, jnp.float32)
    if pieces:
        values = values * shard_levels(own_key, extent, pieces, -0.22, 0.18)
    return jnp.clip(values, -bound, bound).astype(held_as)


def noise_with(own_key, dims, scale, most, cuts, heavy, dtype=jnp.bfloat16):
    entries = scale * jax.random.normal(own_key, dims, jnp.float32)
    if cuts:
        entries = entries * shard_levels(own_key, dims, cuts, -0.22, 0.18)
    return jnp.clip(with_spikes(entries, jax.random.fold_in(own_key, 3), *heavy), -most, most).astype(dtype)


def setup_inputs(seed: int = 0) -> dict:
    key_of = jax.random.split(jax.random.key(seed), 12)
    return {
        "hidden_in": bell_draw(key_of[0], (TOKENS, D), 1.0, 6.0, ((1, 8),)),
        "up_act": bell_draw(key_of[1], (TOKENS, FF), 1.0, 6.0, ((0, 8), (1, 128))),
        "up_val": bell_draw(key_of[2], (TOKENS, FF), 1.0, 6.0, ((0, 8), (1, 128))),
        "cotangent": noise_with(key_of[3], (TOKENS, D), 1.0, 6.0, ((0, 8),), (0, 1, 8, 2.0)),
        "w_act": bell_draw(key_of[4], (D, FF), D ** -0.5, 0.09375, ((0, 8), (1, 128))),
        "w_val": bell_draw(key_of[5], (D, FF), D ** -0.5, 0.09375, ((0, 8), (1, 128))),
        "w_down": bell_draw(key_of[6], (FF, D), FF ** -0.5, 0.0546875, ((0, 128), (1, 8))),
        "conv_act": bell_draw(key_of[7], (KW, FF), 0.577, 3.0, ((1, 128),)),
        "conv_val": bell_draw(key_of[8], (KW, FF), 0.577, 3.0, ((1, 128),)),
        "bias_act": bell_draw(key_of[9], (FF,), 0.5, 3.0, ((0, 128),)),
        "bias_val": bell_draw(key_of[10], (FF,), 0.5, 3.0, ((0, 128),)),
    }


def conv_ahead(upper, taps, bias):
    length = upper.shape[0]
    padded = jnp.concatenate([jnp.zeros((KW - 1, upper.shape[1]), jnp.float32), upper.astype(jnp.float32)], 0)
    total = jnp.zeros(upper.shape, jnp.float32) + bias.astype(jnp.float32)
    for offset in range(KW):
        total = total + taps[offset].astype(jnp.float32) * padded[offset:offset + length]
    return (total, padded)

def conv_behind(grad_pre, taps):
    length = grad_pre.shape[0]
    padded = jnp.concatenate([grad_pre, jnp.zeros((KW - 1, grad_pre.shape[1]), jnp.float32)], 0)
    total = jnp.zeros(grad_pre.shape, jnp.float32)
    for offset in range(KW):
        total = total + taps[offset].astype(jnp.float32) * padded[KW - 1 - offset:KW - 1 - offset + length]
    return total.astype(jnp.bfloat16)

def tap_grads(grad_pre, padded):
    length = grad_pre.shape[0]
    rows = [lax.optimization_barrier(jnp.sum(grad_pre * padded[offset:offset + length], axis=0)) for offset in range(KW)]
    return (jnp.stack(rows, 0), lax.optimization_barrier(jnp.sum(grad_pre, axis=0)))

def reference(hidden_in, up_act, up_val, cotangent, w_act, w_val, w_down, conv_act, conv_val, bias_act, bias_val):
    pre_act, padded_act = conv_ahead(up_act, conv_act, bias_act)
    pre_val, padded_val = conv_ahead(up_val, conv_val, bias_val)
    gelu_act, gelu_back = jax.vjp(jax.nn.gelu, pre_act)
    mixed = (gelu_act * pre_val).astype(jnp.bfloat16)
    grad_mixed = jnp.dot(cotangent, w_down.T, preferred_element_type=jnp.float32).astype(jnp.bfloat16)
    grad_mixed = lax.optimization_barrier(grad_mixed).astype(jnp.float32)
    grad_pre_act = gelu_back(grad_mixed * pre_val)[0]
    grad_pre_val = grad_mixed * gelu_act
    grad_up_act = conv_behind(grad_pre_act, conv_act)
    grad_up_val = conv_behind(grad_pre_val, conv_val)
    grad_conv_act, grad_bias_act = tap_grads(grad_pre_act, padded_act)
    grad_conv_val, grad_bias_val = tap_grads(grad_pre_val, padded_val)
    grad_w_act = jnp.dot(hidden_in.T, grad_up_act, preferred_element_type=jnp.float32)
    grad_w_val = jnp.dot(hidden_in.T, grad_up_val, preferred_element_type=jnp.float32)
    grad_w_down = jnp.dot(mixed.T, cotangent, preferred_element_type=jnp.float32)
    grad_input = jnp.dot(grad_up_act, w_act.T, preferred_element_type=jnp.float32)
    grad_input = grad_input + jnp.dot(grad_up_val, w_val.T, preferred_element_type=jnp.float32)
    grad_input = grad_input.astype(jnp.bfloat16)
    rows_act = lax.optimization_barrier(jnp.sum(grad_w_act * grad_w_act, axis=1))
    rows_val = lax.optimization_barrier(jnp.sum(grad_w_val * grad_w_val, axis=1))
    rows_down = lax.optimization_barrier(jnp.sum(grad_w_down * grad_w_down, axis=1))
    conv_rows = jnp.stack([lax.optimization_barrier(jnp.sum(grad_conv_act * grad_conv_act, axis=1)), lax.optimization_barrier(jnp.sum(grad_conv_val * grad_conv_val, axis=1))], 0)
    return (grad_input, grad_w_act, grad_w_val, grad_w_down, grad_conv_act, grad_conv_val, grad_bias_act, grad_bias_val, rows_act, rows_val, rows_down, conv_rows)
```

```python
import functools

import jax
import jax.numpy as jnp
from jax import lax
from jax.experimental import pallas as pl
from jax.experimental.pallas import tpu as pltpu
from jax.sharding import Mesh
from jax.sharding import PartitionSpec as P

FS = ("fs_0", "fs_1")
TP = ("tp_0", "tp_1")
TP_FS = ("tp_0", "tp_1", "fs_0", "fs_1")
MESH = pl.DeviceIdType.MESH
F32 = jnp.float32
BF16 = jnp.bfloat16
ROOT_2_OVER_PI = 0.7978845608028654
CUBIC = 0.044715


def dot_nn(a, b):
    return lax.dot_general(a, b, (((1,), (0,)), ((), ())), preferred_element_type=F32)


def dot_nt(a, b):
    return lax.dot_general(a, b, (((1,), (1,)), ((), ())), preferred_element_type=F32)


def kernel(
    sizes,
    hid, upa, upv, cot, wa, wv, wd, ca, cv, ba, bv,
    o_gi, o_gwa, o_gwv, o_gwd, o_gca, o_gcv, o_gba, o_gbv, o_ra, o_rv, o_rd, o_cr,
    cotx, hidv, wdall, ea, ev, hpa, hpv, hna, hnv, ga, gv,
    agb, tapb, cotc, lch, wt, ysend, yrecv, acc, zsend, zrecv,
    fsend, frecv, rsend, ryrecv, rzrecv, rfin, drecv,
    lsem, hs, hr, as_, ar, afs, afr, gs, gr, gfs, gfr, ts, tr, cs, cr,
    ys, yr, zs, zr, fs_, fr, r1s, r1r, r2s, r2r, r3s, r3r, ds_, dr,
):
    nz, ny, nx, nc = sizes
    z, y = lax.axis_index("fs_0"), lax.axis_index("fs_1")
    x, c = lax.axis_index("tp_0"), lax.axis_index("tp_1")
    j = x * 2 + c
    rows, hidden = upa.shape
    width = wd.shape[1]
    n = nx * nc
    pend = []

    def send(src, dst, ssem, rsem, device):
        copy = pltpu.make_async_remote_copy(
            src_ref=src, dst_ref=dst, send_sem=ssem, recv_sem=rsem,
            device_id=device, device_id_type=MESH,
        )
        copy.start()
        pend.append(copy)
        return copy

    cot_in = pltpu.make_async_copy(cot, cotx.at[pl.ds(0, rows)], lsem.at[0])
    cot_in.start()
    hid_in = pltpu.make_async_copy(hid, hidv, lsem.at[1])
    hid_in.start()

    barrier = pltpu.get_barrier_semaphore()

    def tp_device(k):
        other = lax.rem(j + k, n)
        return {"tp_0": other // nc, "tp_1": lax.rem(other, nc)}

    for k in range(1, n):
        pl.semaphore_signal(barrier, inc=1, device_id=tp_device(k), device_id_type=MESH)
    for k in range(1, ny):
        pl.semaphore_signal(barrier, inc=1, device_id={"fs_1": lax.rem(y + k, ny)}, device_id_type=MESH)
    for k in range(1, nz):
        pl.semaphore_signal(barrier, inc=1, device_id={"fs_0": lax.rem(z + k, nz)}, device_id_type=MESH)
    pl.semaphore_wait(barrier, n - 1 + ny - 1 + nz - 1)

    partner = {"tp_1": 1 - c}

    def chip(dx):
        return {"tp_0": lax.rem(x + dx, nx)}

    def slot_of(dx, core):
        return lax.rem(x + nx - dx, nx) * 2 + core

    near = (1, 3, 2)
    a_copy = {}
    for dx in near:
        a_copy[dx] = send(wd, wdall.at[j], as_.at[dx], ar.at[dx], chip(dx))
    a_copy[0] = send(wd, wdall.at[j], as_.at[0], ar.at[0], partner)
    up_dev, down_dev = tp_device(1), tp_device(n - 1)
    h_copy = [
        send(cot.at[pl.ds(0, 8)], cotx.at[pl.ds(rows, 8)], hs.at[0], hr.at[0], down_dev),
        send(upa.at[pl.ds(0, 8)], hna, hs.at[1], hr.at[1], down_dev),
        send(upv.at[pl.ds(0, 8)], hnv, hs.at[2], hr.at[2], down_dev),
        send(upa.at[pl.ds(rows - 8, 8)], hpa, hs.at[3], hr.at[3], up_dev),
        send(upv.at[pl.ds(rows - 8, 8)], hpv, hs.at[4], hr.at[4], up_dev),
    ]

    eye = (
        lax.broadcasted_iota(jnp.int32, (hidden, hidden), 0)
        == lax.broadcasted_iota(jnp.int32, (hidden, hidden), 1)
    ).astype(F32).astype(BF16)
    wt[pl.ds(0, hidden), :] = dot_nt(eye, wa[...]).astype(BF16)
    wt[pl.ds(hidden, hidden), :] = dot_nt(eye, wv[...]).astype(BF16)
    out_row = lax.broadcasted_iota(jnp.int32, (rows, rows), 0)
    in_row = lax.broadcasted_iota(jnp.int32, (rows, rows), 1)
    order = (in_row == lax.rem(out_row, nz) * ny + out_row // nz).astype(F32).astype(BF16)

    for copy in h_copy:
        copy.wait_recv()
    first = (j > 0).astype(F32)
    last = (j < n - 1).astype(F32)
    taps_a, taps_v = ca[...].astype(F32), cv[...].astype(F32)
    ext = 8 + rows + 8
    for e, hp, up, hn in ((ea, hpa, upa, hna), (ev, hpv, upv, hnv)):
        e[pl.ds(0, 8), :] = hp[...].astype(F32) * first
        e[pl.ds(8, rows), :] = up[...].astype(F32)
        e[pl.ds(8 + rows, 8), :] = hn[...].astype(F32)
    full = rows + 8

    def ahead(e, taps, bias):
        total = bias[...].astype(F32).reshape(1, hidden) + taps[0:1] * e[pl.ds(6, full), :]
        total = total + taps[1:2] * e[pl.ds(7, full), :]
        return total + taps[2:3] * e[pl.ds(8, full), :]

    pre_a = ahead(ea, taps_a, ba)
    pre_v = ahead(ev, taps_v, bv)
    square = pre_a * pre_a
    th = jnp.tanh(ROOT_2_OVER_PI * (pre_a + CUBIC * pre_a * square))
    half = 0.5 * (1.0 + th)
    gelu = pre_a * half
    slope = half + 0.5 * pre_a * (1.0 - th * th) * (ROOT_2_OVER_PI * (1.0 + 3.0 * CUBIC * square))
    ga[...] = pre_v * slope
    gv[...] = gelu
    mixed = (gelu * pre_v)[0:rows]
    agb[j, pl.ds(2 * hidden, hidden), :] = mixed.T.astype(BF16)

    cot_in.wait()

    def part(slot, block):
        return dot_nt(cotx[:, pl.ds(pl.multiple_of(slot * width, width), width)], block)

    gm = part(j, wd[...])
    a_copy[0].wait_recv()
    gm = gm + part(x * 2 + 1 - c, wdall[x * 2 + 1 - c])
    f_copy = {}
    for dx in near:
        a_copy[dx].wait_recv()
        s = slot_of(dx, c)
        f_copy[dx] = send(wdall.at[s], wdall.at[s], afs.at[dx], afr.at[dx], partner)
        gm = gm + part(s, wdall[s])
    for dx in near:
        f_copy[dx].wait_recv()
        s = slot_of(dx, 1 - c)
        gm = gm + part(s, wdall[s])
    gm = gm.astype(BF16).astype(F32)
    row = lax.broadcasted_iota(jnp.int32, (full, hidden), 0)
    gm = jnp.where(row < rows, gm, gm * last)
    ga[...] = gm * ga[...]
    gv[...] = gm * gv[...]

    def behind(g, taps):
        total = taps[0:1] * g[pl.ds(2, rows), :] + taps[1:2] * g[pl.ds(1, rows), :]
        return total + taps[2:3] * g[pl.ds(0, rows), :]

    agb[j, pl.ds(0, hidden), :] = behind(ga, taps_a).T.astype(BF16)
    agb[j, pl.ds(hidden, hidden), :] = behind(gv, taps_v).T.astype(BF16)
    g_copy = {}
    for dx in near:
        g_copy[dx] = send(agb.at[j], agb.at[j], gs.at[dx], gr.at[dx], chip(dx))
    g_copy[0] = send(agb.at[j], agb.at[j], gs.at[0], gr.at[0], partner)

    at_row = 0
    tapb[j] = jnp.zeros((8, 128), F32)
    for g, e in ((ga, ea), (gv, ev)):
        grad = g[pl.ds(0, rows), :]
        for k in range(3):
            tapb[j, pl.ds(at_row, 1), pl.ds(0, hidden)] = jnp.sum(
                grad * e[pl.ds(6 + k, rows), :], axis=0, keepdims=True
            )
            at_row += 1
        tapb[j, pl.ds(at_row, 1), pl.ds(0, hidden)] = jnp.sum(grad, axis=0, keepdims=True)
        at_row += 1
    t_copy = [
        send(tapb.at[j], tapb.at[j], ts.at[k], tr.at[k], tp_device(k)) for k in range(1, n)
    ]

    def arrange(s):
        ordered = dot_nt(order, agb[s, pl.ds(0, 2 * hidden), :]).astype(BF16)
        for k in range(ny):
            lch[k, pl.ds(pl.multiple_of(s * nz, nz), nz), :] = ordered[k * nz : (k + 1) * nz]

    arrange(j)
    g_copy[0].wait_recv()
    arrange(x * 2 + 1 - c)
    gf_copy = {}
    for dx in near:
        g_copy[dx].wait_recv()
        s = slot_of(dx, c)
        gf_copy[dx] = send(agb.at[s], agb.at[s], gfs.at[dx], gfr.at[dx], partner)
        arrange(s)
    for dx in near:
        gf_copy[dx].wait_recv()
        arrange(slot_of(dx, 1 - c))

    c_copy = []
    for k in range(1, n):
        other = lax.rem(j + k, n)
        c_copy.append(
            send(
                cotx.at[pl.ds(0, rows), pl.ds(pl.multiple_of(other * width, width), width)],
                cotc.at[j], cs.at[k], cr.at[k], tp_device(k),
            )
        )

    wt_all = wt[...]
    wide = width // 2

    def mine(k):
        return dot_nn(lch[lax.rem(y + k + ny, ny)], wt_all)

    def pass_on(i, value, step):
        ysend[i] = value.astype(BF16)
        return send(
            ysend.at[i], yrecv.at[i], ys.at[i], yr.at[i], {"fs_1": lax.rem(y + step + ny, ny)}
        )

    ring = {}

    def arrived(i):
        ring[i].wait_recv()
        return yrecv[i].astype(F32)

    t = mine(4)
    ring[0] = pass_on(0, t[:, :wide], 1)
    ring[7] = pass_on(7, t[:, wide:], -1)
    tp, tm = mine(3), mine(-3)
    ring[4] = pass_on(4, tp[:, wide:], 1)
    ring[11] = pass_on(11, tm[:, :wide], -1)

    hid_in.wait()
    gathered = jnp.concatenate([agb[s, pl.ds(0, 2 * hidden), :] for s in range(n)], axis=1)
    gwt = dot_nn(gathered, hidv[...])
    ring[1] = pass_on(1, arrived(0) + tp[:, :wide], 1)
    ring[8] = pass_on(8, arrived(7) + tm[:, wide:], -1)
    o_gwa[...] = gwt[0:hidden].T
    o_gwv[...] = gwt[hidden:].T
    squares = gwt * gwt
    row_a = jnp.sum(squares[0:hidden], axis=0, keepdims=True)
    row_v = jnp.sum(squares[hidden:], axis=0, keepdims=True)
    tp, tm = mine(2), mine(-2)
    ring[5] = pass_on(5, arrived(4) + tp[:, wide:], 1)
    ring[12] = pass_on(12, arrived(11) + tm[:, :wide], -1)
    for copy in t_copy:
        copy.wait_recv()
    taps = tapb[0]
    for s in range(1, n):
        taps = taps + tapb[s]
    taps = taps[:, 0:hidden]
    o_gca[...] = taps[0:3]
    o_gba[...] = taps[3:4]
    o_gcv[...] = taps[4:7]
    o_gbv[...] = taps[7:8]
    sums = jnp.sum(taps * taps, axis=1, keepdims=True)
    spot = lax.broadcasted_iota(jnp.int32, (8, 128), 0) == lax.broadcasted_iota(
        jnp.int32, (8, 128), 1
    )
    conv_row = jnp.sum(jnp.where(spot, sums, 0.0), axis=0, keepdims=True)
    for k in range(ny):
        source = row_a if k < ny // 2 else row_v
        lane = (k % (ny // 2)) * 128
        rsend[k, pl.ds(0, 1), :] = source[:, lane : lane + 128]
        rsend[k, pl.ds(1, 1), :] = conv_row
    r1_copy = []
    for k in range(1, ny):
        other = lax.rem(y + k, ny)
        r1_copy.append(
            send(rsend.at[other], ryrecv.at[y], r1s.at[k], r1r.at[k], {"fs_1": other})
        )
    ryrecv[y] = rsend[y]
    ring[2] = pass_on(2, arrived(1) + tp[:, :wide], 1)
    ring[9] = pass_on(9, arrived(8) + tm[:, wide:], -1)
    tp, tm = mine(1), mine(-1)
    ring[6] = pass_on(6, arrived(5) + tp[:, wide:], 1)
    ring[13] = pass_on(13, arrived(12) + tm[:, :wide], -1)
    ring[3] = pass_on(3, arrived(2) + tp[:, :wide], 1)
    ring[10] = pass_on(10, arrived(9) + tm[:, wide:], -1)
    for copy in r1_copy:
        copy.wait_recv()
    piece = ryrecv[0]
    for s in range(1, ny):
        piece = piece + ryrecv[s]
    rzrecv[z] = piece
    r2_copy = [
        send(rzrecv.at[z], rzrecv.at[z], r2s.at[k], r2r.at[k], {"fs_0": lax.rem(z + k, nz)})
        for k in range(1, nz)
    ]
    t = mine(0)
    lanes_b = t[:, wide:] + (arrived(6) + arrived(10))
    lanes_a = t[:, :wide] + (arrived(13) + arrived(3))
    tiles = width // 128
    for k in range(tiles // 2):
        acc[k] = lanes_a[:, 128 * k : 128 * (k + 1)]
        acc[tiles // 2 + k] = lanes_b[:, 128 * k : 128 * (k + 1)]

    for k in range(nz):
        for i in range(tiles):
            zsend[k, :, pl.ds(128 * i, 128)] = acc[i, pl.ds(k, n, stride=nz), :].astype(BF16)
    z_copy = []
    for k in range(1, nz):
        other = lax.rem(z + k, nz)
        z_copy.append(send(zsend.at[other], zrecv.at[z], zs.at[k], zr.at[k], {"fs_0": other}))
    zrecv[z] = zsend[z]

    for copy in c_copy:
        copy.wait_recv()
    cotc[j] = cotx[pl.ds(0, rows), pl.ds(pl.multiple_of(j * width, width), width)]
    mixed_all = jnp.concatenate([agb[s, pl.ds(2 * hidden, hidden), :] for s in range(n)], axis=1)
    gwd = dot_nn(mixed_all, cotc[...].reshape(n * rows, width))
    o_gwd[...] = gwd
    sq = gwd * gwd
    lanes = sq[:, 0:128]
    for k in range(1, width // 128):
        lanes = lanes + sq[:, 128 * k : 128 * (k + 1)]
    drecv[j] = jnp.zeros((1, 128), F32)
    drecv[j, :, pl.ds(0, hidden)] = jnp.sum(lanes.T, axis=0, keepdims=True)
    d_copy = [
        send(drecv.at[j], drecv.at[j], ds_.at[k], dr.at[k], tp_device(k)) for k in range(1, n)
    ]

    for copy in r2_copy:
        copy.wait_recv()
    piece = rzrecv[0]
    for s in range(1, nz):
        piece = piece + rzrecv[s]
    rfin[y] = piece
    r3_copy = [
        send(rfin.at[y], rfin.at[y], r3s.at[k], r3r.at[k], {"fs_1": lax.rem(y + k, ny)})
        for k in range(1, ny)
    ]
    o_cr[...] = piece[1:2]

    for copy in z_copy:
        copy.wait_recv()
    total = zrecv[0].astype(F32)
    for s in range(1, nz):
        total = total + zrecv[s].astype(F32)
    for s in range(n):
        fsend[s] = total[s : s + 1]
    f2_copy = []
    for k in range(1, n):
        other = lax.rem(j + k, n)
        f2_copy.append(send(fsend.at[other], frecv.at[j], fs_.at[k], fr.at[k], tp_device(k)))
    frecv[j] = fsend[j]

    for copy in d_copy:
        copy.wait_recv()
    down = drecv[0]
    for s in range(1, n):
        down = down + drecv[s]
    o_rd[...] = down
    for copy in r3_copy:
        copy.wait_recv()
    half_n = ny // 2
    for k in range(half_n):
        o_ra[:, pl.ds(128 * k, 128)] = rfin[k, pl.ds(0, 1), :]
        o_rv[:, pl.ds(128 * k, 128)] = rfin[half_n + k, pl.ds(0, 1), :]
    for copy in f2_copy:
        copy.wait_recv()
    for s in range(n):
        o_gi[:, pl.ds(width * s, width)] = frecv[s].astype(BF16)
    for copy in pend:
        copy.wait_send()


def per_device(sizes, hid, upa, upv, cot, wa, wv, wd, ca, cv, ba, bv):
    nz, ny, nx, nc = sizes
    n = nx * nc
    rows, hidden = upa.shape
    width = wd.shape[1]
    tokens = hid.shape[0]
    vm = pl.BlockSpec(memory_space=pltpu.VMEM)
    hbm = pl.BlockSpec(memory_space=pl.ANY)
    dma = pltpu.SemaphoreType.DMA

    def f32(*shape):
        return jax.ShapeDtypeStruct(shape, F32)

    outs = (
        jax.ShapeDtypeStruct((1, n * width), BF16),
        f32(width, hidden), f32(width, hidden), f32(hidden, width),
        f32(3, hidden), f32(3, hidden), f32(1, hidden), f32(1, hidden),
        f32(1, width), f32(1, width), f32(1, 128), f32(1, 128),
    )
    v = pltpu.VMEM
    scratch = [
        v((rows + 8, n * width), BF16), v((tokens, width), BF16), v((n, hidden, width), BF16),
        v((rows + 16, hidden), F32), v((rows + 16, hidden), F32),
        v((8, hidden), BF16), v((8, hidden), BF16), v((8, hidden), BF16), v((8, hidden), BF16),
        v((rows + 8, hidden), F32), v((rows + 8, hidden), F32),
        v((n, 3 * hidden, rows), BF16), v((n, 8, 128), F32), v((n, rows, width), BF16),
        v((ny, rows, 2 * hidden), BF16), v((2 * hidden, width), BF16),
        v((14, rows, width // 2), BF16), v((14, rows, width // 2), BF16),
        v((width // 128, rows, 128), F32), v((nz, n, width), BF16), v((nz, n, width), BF16),
        v((n, 1, width), F32), v((n, 1, width), F32),
        v((ny, 2, 128), F32), v((ny, 2, 128), F32), v((nz, 2, 128), F32), v((ny, 2, 128), F32),
        v((n, 1, 128), F32),
        dma((2,)), dma((5,)), dma((5,)), dma((4,)), dma((4,)), dma((4,)), dma((4,)),
        dma((4,)), dma((4,)), dma((4,)), dma((4,)), dma((n,)), dma((n,)), dma((n,)), dma((n,)),
        dma((14,)), dma((14,)), dma((nz,)), dma((nz,)), dma((n,)), dma((n,)),
        dma((ny,)), dma((ny,)), dma((nz,)), dma((nz,)), dma((ny,)), dma((ny,)),
        dma((n,)), dma((n,)),
    ]
    res = pl.pallas_call(
        functools.partial(kernel, sizes),
        out_shape=outs,
        in_specs=[hbm, vm, vm, hbm, vm, vm, vm, vm, vm, vm, vm],
        out_specs=[vm] * len(outs),
        scratch_shapes=scratch,
        compiler_params=pltpu.CompilerParams(
            collective_id=0, has_side_effects=True, vmem_limit_bytes=48 * 1024 * 1024
        ),
    )(hid, upa, upv, cot, wa, wv, wd, ca, cv, ba, bv)
    gi, gwa, gwv, gwd, gca, gcv, gba, gbv, ra, rv, rd, cr = res
    conv_rows = jnp.stack([cr[0, 0:3], cr[0, 4:7]], 0)
    return (
        gi, gwa, gwv, gwd, gca, gcv, gba[0], gbv[0], ra[0], rv[0], rd[0, :hidden], conv_rows,
    )


def solution(mesh):
    sizes = (16, 8, 4, 2)
    finer = Mesh(mesh.devices.reshape(sizes), FS + TP)
    return jax.shard_map(
        functools.partial(per_device, sizes),
        mesh=finer,
        in_specs=(
            P(None, TP), P(TP, FS), P(TP, FS), P(TP, None), P(TP, FS), P(TP, FS),
            P(FS, TP), P(None, FS), P(None, FS), P(FS), P(FS),
        ),
        out_specs=(
            P(TP_FS, None), P(TP, FS), P(TP, FS), P(FS, TP), P(None, FS), P(None, FS),
            P(FS), P(FS), P(TP), P(TP), P(FS), P(),
        ),
        check_vma=False,
    )
```

```python
import functools

import jax
import jax.numpy as jnp
from jax import lax
from jax.experimental import pallas as pl
from jax.experimental.pallas import tpu as pltpu
from jax.sharding import Mesh
from jax.sharding import PartitionSpec as P

FS = ("fs_0", "fs_1")
TP = ("tp_0", "tp_1")
TP_FS = ("tp_0", "tp_1", "fs_0", "fs_1")
MESH = pl.DeviceIdType.MESH
F32 = jnp.float32
BF16 = jnp.bfloat16
ROOT_2_OVER_PI = 0.7978845608028654
CUBIC = 0.044715


def dot_nn(a, b):
    return lax.dot_general(a, b, (((1,), (0,)), ((), ())), preferred_element_type=F32)


def dot_nt(a, b):
    return lax.dot_general(a, b, (((1,), (1,)), ((), ())), preferred_element_type=F32)


def kernel(
    sizes,
    hid, upa, upv, cot, wa, wv, wd, ca, cv, ba, bv,
    o_gi, o_gwa, o_gwv, o_gwd, o_tap, o_ra, o_rv, o_rd, o_cr,
    cotx, hidv, wdall, wall, uas, uvs, cas, cvs, bas, bvs, hb, hprev, hnext,
    agb, tapb, cotc, relay, pbuf, ysend, yrecv, acc, zsend, zrecv, row_out,
    rz, ry, drecv,
    lsem, hs, hr, wds_, wdr, was, war, wvs, wvr, gs, gr, ts, tr, cs, cr,
    ys, yr, zs, zr, r1s, r1r, r2s, r2r, ds_, dr,
):
    nz, ny, nx, nc = sizes
    z, y = lax.axis_index("fs_0"), lax.axis_index("fs_1")
    x, c = lax.axis_index("tp_0"), lax.axis_index("tp_1")
    j = x * 2 + c
    hidden, rows = upa.shape
    width = wd.shape[1]
    n = nx * nc
    pend = []

    def send(src, dst, ssem, rsem, device):
        copy = pltpu.make_async_remote_copy(
            src_ref=src, dst_ref=dst, send_sem=ssem, recv_sem=rsem,
            device_id=device, device_id_type=MESH,
        )
        copy.start()
        pend.append(copy)
        return copy

    barrier = pltpu.get_barrier_semaphore()

    def tp_device(k):
        other = lax.rem(j + k, n)
        return {"tp_0": other // nc, "tp_1": lax.rem(other, nc)}

    for k in range(1, nz):
        pl.semaphore_signal(barrier, inc=1, device_id={"fs_0": lax.rem(z + k, nz)}, device_id_type=MESH)
    for k in range(1, ny):
        pl.semaphore_signal(barrier, inc=1, device_id={"fs_1": lax.rem(y + k, ny)}, device_id_type=MESH)
    for k in range(1, n):
        pl.semaphore_signal(barrier, inc=1, device_id=tp_device(k), device_id_type=MESH)

    loads = []
    for i, (src, dst) in enumerate((
        (wd, wdall.at[j]), (upa, uas), (upv, uvs), (ca, cas), (cv, cvs), (ba, bas), (bv, bvs),
        (cot, cotx.at[pl.ds(0, rows)]), (wa, wall.at[j, pl.ds(0, hidden)]),
        (wv, wall.at[j, pl.ds(hidden, hidden)]), (hid, hidv),
    )):
        copy = pltpu.make_async_copy(src, dst, lsem.at[i])
        copy.start()
        loads.append(copy)
    for copy in loads[0:7]:
        copy.wait()

    lane = lax.broadcasted_iota(jnp.int32, (hidden, rows), 1)

    def roll(value, by):
        return pltpu.roll(value, by % rows, 1)

    ua, uv = uas[...].astype(F32), uvs[...].astype(F32)
    heads = jnp.where(lane < 2, ua, roll(uv, 2))
    tails = jnp.where(lane >= rows - 2, ua, roll(uv, -2))
    hb[...] = jnp.where(lane < rows // 2, heads, tails).astype(BF16)

    pl.semaphore_wait(barrier, n - 1 + ny - 1 + nz - 1)

    partner = {"tp_1": 1 - c}

    def chip(dx):
        return {"tp_0": lax.rem(x + dx, nx)}

    def slot_of(dx, core):
        return lax.rem(x + nx - dx, nx) * 2 + core

    slots = (
        j, x * 2 + 1 - c, slot_of(1, c), slot_of(3, c),
        slot_of(1, 1 - c), slot_of(3, 1 - c), slot_of(2, c), slot_of(2, 1 - c),
    )

    class Gather:
        def __init__(self, buf, first, count, ssem, rsem):
            self.buf, self.first, self.count, self.half = buf, first, count, count // 2
            self.ssem, self.rsem, self.copies = ssem, rsem, {}

        def go(self, i, slot, at, size, device):
            view = self.buf.at[slot, pl.ds(self.first + at, size)]
            self.copies[i] = send(view, view, self.ssem.at[i], self.rsem.at[i], device)

        def start(self):
            self.go(1, j, 0, self.count, chip(1))
            self.go(2, j, 0, self.count, chip(3))
            self.go(0, j, 0, self.count, partner)

        def wait(self, *which):
            for i in which:
                self.copies[i].wait_recv()

        def pass_near(self):
            self.wait(1)
            self.go(3, slots[2], 0, self.half, chip(1))
            self.go(5, slots[2], 0, self.count, partner)
            self.wait(2)
            self.go(4, slots[3], self.half, self.half, chip(3))
            self.go(6, slots[3], 0, self.count, partner)

        def pass_far(self):
            self.wait(3)
            self.go(7, slots[6], 0, self.half, partner)
            self.wait(4)
            self.go(8, slots[6], self.half, self.half, partner)

    down_all = Gather(wdall, 0, hidden, wds_, wdr)
    act_all = Gather(wall, 0, hidden, was, war)
    val_all = Gather(wall, hidden, hidden, wvs, wvr)
    grads_all = Gather(agb, 0, 3 * hidden, gs, gr)
    down_all.start()
    up_dev, down_dev = tp_device(1), tp_device(n - 1)
    h_copy = [
        send(cot.at[pl.ds(0, 8)], cotx.at[pl.ds(rows, 8)], hs.at[0], hr.at[0], down_dev),
        send(hb, hnext, hs.at[1], hr.at[1], down_dev),
        send(hb, hprev, hs.at[2], hr.at[2], up_dev),
    ]

    for copy in loads[8:10]:
        copy.wait()
    act_all.start()

    out_row = lax.broadcasted_iota(jnp.int32, (rows, rows), 0)
    in_row = lax.broadcasted_iota(jnp.int32, (rows, rows), 1)
    order = (in_row == lax.rem(out_row, nz) * ny + out_row // nz).astype(F32).astype(BF16)
    table = jnp.concatenate(
        [cas[...].astype(F32), bas[...].astype(F32).reshape(1, hidden),
         cvs[...].astype(F32), bvs[...].astype(F32).reshape(1, hidden)], axis=0,
    ).T
    par_a = [table[:, k : k + 1] for k in range(4)]
    par_v = [table[:, k : k + 1] for k in range(4, 8)]

    for copy in h_copy:
        copy.wait_recv()
    first = (j > 0).astype(F32)
    last = (j < n - 1).astype(F32)
    before = hprev[...].astype(F32) * first
    after = hnext[...].astype(F32)

    def ahead(par, u2, u1, u0):
        return par[3] + par[0] * u2 + par[1] * u1 + par[2] * u0

    def shifted(u, prev):
        u1 = jnp.where(lane < 1, roll(prev, 1), roll(u, 1))
        return jnp.where(lane < 2, roll(prev, 2), roll(u, 2)), u1, u

    def shifted_next(u, following):
        u1 = jnp.where(lane < 1, roll(u, 1), roll(following, 1))
        return [v[:, 0:8] for v in (roll(u, 2), u1, following)]

    ups_a = shifted(ua, before)
    ups_v = shifted(uv, roll(before, 2))
    next_a = shifted_next(ua, after)
    next_v = shifted_next(uv, roll(after, -2))

    def activation(pre_a, pre_v):
        square = pre_a * pre_a
        th = jnp.tanh(ROOT_2_OVER_PI * (pre_a + CUBIC * pre_a * square))
        half = 0.5 * (1.0 + th)
        gelu = pre_a * half
        slope = half + 0.5 * pre_a * (1.0 - th * th) * (ROOT_2_OVER_PI * (1.0 + 3.0 * CUBIC * square))
        return pre_v * slope, gelu, gelu * pre_v

    fac_a, fac_v, mixed = activation(ahead(par_a, *ups_a), ahead(par_v, *ups_v))
    nfac_a, nfac_v, _ = activation(ahead(par_a, *next_a), ahead(par_v, *next_v))
    agb[j, pl.ds(2 * hidden, hidden), :] = mixed.astype(BF16)

    loads[7].wait()

    def part(slot, block):
        return dot_nt(block, cotx[:, pl.ds(pl.multiple_of(slot * width, width), width)])

    gm = part(j, wdall[j])
    down_all.wait(0)
    gm = gm + part(slots[1], wdall[slots[1]])
    down_all.pass_near()
    val_all.start()
    gm = gm + part(slots[2], wdall[slots[2]]) + part(slots[3], wdall[slots[3]])
    down_all.wait(5, 6)
    gm = gm + part(slots[4], wdall[slots[4]]) + part(slots[5], wdall[slots[5]])
    act_all.pass_near()
    down_all.pass_far()
    gm = gm + part(slots[6], wdall[slots[6]])
    down_all.wait(7, 8)
    gm = gm + part(slots[7], wdall[slots[7]])
    gm = gm.astype(BF16).astype(F32)
    gm_next = gm[:, rows:] * last
    gm = gm[:, 0:rows]
    grad_a, grad_v = gm * fac_a, gm * fac_v
    empty = jnp.zeros((hidden, rows - 8), F32)
    after_a = jnp.concatenate([gm_next * nfac_a, empty], axis=1)
    after_v = jnp.concatenate([gm_next * nfac_v, empty], axis=1)

    def behind(par, grad, following):
        g1 = jnp.where(lane < rows - 1, roll(grad, -1), roll(following, -1))
        g2 = jnp.where(lane < rows - 2, roll(grad, -2), roll(following, -2))
        return par[0] * g2 + par[1] * g1 + par[2] * grad

    agb[j, pl.ds(0, hidden), :] = behind(par_a, grad_a, after_a).astype(BF16)
    agb[j, pl.ds(hidden, hidden), :] = behind(par_v, grad_v, after_v).astype(BF16)
    val_all.pass_near()
    grads_all.start()
    left = dot_nt(order, agb[j, pl.ds(0, 2 * hidden), :]).astype(BF16)

    spread = jnp.zeros((hidden, rows), F32)
    at = 0
    for grad, ups in ((grad_a, ups_a), (grad_v, ups_v)):
        for k in range(4):
            terms = grad * ups[k] if k < 3 else grad
            spread = jnp.where(lane == at, jnp.sum(terms, axis=1, keepdims=True), spread)
            at += 1
    tapb[j] = spread.T[0:8]
    t_copy = [
        send(tapb.at[j], tapb.at[j], ts.at[k], tr.at[k], tp_device(k)) for k in range(1, n)
    ]

    def product(a):
        pbuf[a] = dot_nn(left, wall[slots[a]])

    def mine(k, half):
        at = pl.multiple_of(lax.rem(y + k + ny, ny) * nz, nz)
        return pbuf[pl.ds(4 * half, 4), pl.ds(at, nz), :]

    ring = {}

    def pass_on(i, value, step):
        ysend[i] = value.astype(BF16)
        ring[i] = send(
            ysend.at[i], yrecv.at[i], ys.at[i], yr.at[i], {"fs_1": lax.rem(y + step + ny, ny)}
        )

    def arrived(i):
        ring[i].wait_recv()
        return yrecv[i].astype(F32)

    product(0)
    act_all.wait(0)
    val_all.wait(0)
    product(1)
    product(2)
    product(3)
    pass_on(0, mine(4, 0), 1)
    pass_on(11, mine(-3, 0), -1)
    act_all.wait(5, 6)
    val_all.wait(5, 6)
    product(4)
    product(5)
    act_all.pass_far()
    val_all.pass_far()
    product(6)
    act_all.wait(7, 8)
    val_all.wait(7, 8)
    product(7)
    pass_on(7, mine(-4, 1), -1)
    pass_on(4, mine(3, 1), 1)
    grads_all.pass_near()
    pass_on(1, arrived(0) + mine(3, 0), 1)
    pass_on(12, arrived(11) + mine(-2, 0), -1)

    def columns(dx, core):
        at = (lax.rem(x + dx, nx) * 2 + core) * width
        return cotx.at[pl.ds(0, rows), pl.ds(pl.multiple_of(at, width), width)]

    c_copy = [
        send(columns(2, 1 - c), relay, cs.at[6], cr.at[6], {"tp_0": lax.rem(x + 3, nx), "tp_1": 1 - c})
    ]
    for i, (dx, core) in enumerate(((1, c), (3, c), (2, c), (1, 1 - c), (3, 1 - c), (0, 1 - c))):
        c_copy.append(
            send(
                columns(dx, core), cotc.at[j], cs.at[i], cr.at[i],
                {"tp_0": lax.rem(x + dx, nx), "tp_1": core},
            )
        )
    pass_on(8, arrived(7) + mine(-3, 1), -1)
    pass_on(5, arrived(4) + mine(2, 1), 1)
    pass_on(2, arrived(1) + mine(2, 0), 1)
    pass_on(13, arrived(12) + mine(-1, 0), -1)

    grads_all.wait(0, 5, 6)
    grads_all.pass_far()
    grads_all.wait(7, 8)
    loads[10].wait()
    gathered = jnp.concatenate([agb[s, pl.ds(0, 2 * hidden), :] for s in range(n)], axis=1)
    gwt = dot_nn(gathered, hidv[...])
    o_gwa[...] = gwt[0:hidden]
    o_gwv[...] = gwt[hidden:]
    squares = gwt * gwt
    row_a = jnp.sum(squares[0:hidden], axis=0, keepdims=True)
    row_v = jnp.sum(squares[hidden:], axis=0, keepdims=True)
    for copy in t_copy:
        copy.wait_recv()
    taps = tapb[0]
    for s in range(1, n):
        taps = taps + tapb[s]
    o_tap[...] = taps
    sums = jnp.sum(taps * taps, axis=1, keepdims=True)
    spot = lax.broadcasted_iota(jnp.int32, (8, 128), 0) == lax.broadcasted_iota(
        jnp.int32, (8, 128), 1
    )
    tiles = width // 128
    for k in range(tiles):
        rz[z, k] = row_a[:, 128 * k : 128 * (k + 1)]
        rz[z, tiles + k] = row_v[:, 128 * k : 128 * (k + 1)]
    rz[z, 2 * tiles] = jnp.sum(jnp.where(spot, sums, 0.0), axis=0, keepdims=True)
    r1_copy = [
        send(rz.at[z], rz.at[z], r1s.at[k], r1r.at[k], {"fs_0": lax.rem(z + k, nz)})
        for k in range(1, nz)
    ]

    pass_on(9, arrived(8) + mine(-2, 1), -1)
    pass_on(6, arrived(5) + mine(1, 1), 1)
    pass_on(3, arrived(2) + mine(1, 0), 1)
    c_copy[0].wait_recv()
    c_copy.append(send(relay, cotc.at[slot_of(3, 1 - c)], cs.at[7], cr.at[7], chip(3)))
    pass_on(10, arrived(9) + mine(-1, 1), -1)
    for half, (i, k) in enumerate(((13, 3), (6, 10))):
        total = mine(0, half) + (arrived(i) + arrived(k))
        for b in range(4):
            for t in range(tiles):
                acc[t, pl.ds((4 * half + b) * nz, nz), :] = total[b, :, 128 * t : 128 * (t + 1)]

    for k in range(nz):
        for t in range(tiles):
            zsend[k, :, pl.ds(128 * t, 128)] = acc[t, pl.ds(k, n, stride=nz), :].astype(BF16)
    z_copy = []
    for k in range(1, nz):
        other = lax.rem(z + k, nz)
        z_copy.append(send(zsend.at[other], zrecv.at[z], zs.at[k], zr.at[k], {"fs_0": other}))
    zrecv[z] = zsend[z]

    for copy in r1_copy:
        copy.wait_recv()
    piece = rz[0]
    for s in range(1, nz):
        piece = piece + rz[s]
    ry[y] = piece
    r2_copy = [
        send(ry.at[y], ry.at[y], r2s.at[k], r2r.at[k], {"fs_1": lax.rem(y + k, ny)})
        for k in range(1, ny)
    ]

    for copy in c_copy[1:]:
        copy.wait_recv()
    cotc[j] = cotx[pl.ds(0, rows), pl.ds(pl.multiple_of(j * width, width), width)]
    mixed_all = jnp.concatenate([agb[s, pl.ds(2 * hidden, hidden), :] for s in range(n)], axis=1)
    gwd = dot_nn(mixed_all, cotc[...].reshape(n * rows, width))
    o_gwd[...] = gwd
    sq = gwd * gwd
    lanes = sq[:, 0:128]
    for k in range(1, tiles):
        lanes = lanes + sq[:, 128 * k : 128 * (k + 1)]
    drecv[j] = jnp.sum(lanes.T, axis=0, keepdims=True)
    d_copy = [
        send(drecv.at[j], drecv.at[j], ds_.at[k], dr.at[k], tp_device(k)) for k in range(1, n)
    ]

    for copy in r2_copy:
        copy.wait_recv()
    piece = ry[0]
    for s in range(1, ny):
        piece = piece + ry[s]
    for k in range(tiles):
        o_ra[:, pl.ds(128 * k, 128)] = piece[k]
        o_rv[:, pl.ds(128 * k, 128)] = piece[tiles + k]
    o_cr[...] = piece[2 * tiles]
    for copy in d_copy:
        copy.wait_recv()
    down = drecv[0]
    for s in range(1, n):
        down = down + drecv[s]
    o_rd[...] = down

    for copy in z_copy:
        copy.wait_recv()
    total = zrecv[0].astype(F32)
    for s in range(1, nz):
        total = total + zrecv[s].astype(F32)
    for a in range(n):
        row_out[slots[a]] = total[a : a + 1]
    for s in range(n):
        o_gi[:, pl.ds(width * s, width)] = row_out[s].astype(BF16)
    for copy in pend:
        copy.wait_send()


def finish(gi, gwa, gwv, gwd, tap, ra, rv, rd, cr,
           o_gi, o_gwa, o_gwv, o_gwd, o_gca, o_gcv, o_gba, o_gbv, o_ra, o_rv, o_rd, o_cr,
           csem):
    copies = [
        pltpu.make_async_copy(src, dst, csem.at[i])
        for i, (src, dst) in enumerate(((gwa, o_gwa), (gwv, o_gwv), (gwd, o_gwd)))
    ]
    for copy in copies:
        copy.start()
    o_gi[...] = gi[...]
    taps = tap[...]
    o_gca[...] = taps[0:3]
    o_gba[...] = taps[3:4]
    o_gcv[...] = taps[4:7]
    o_gbv[...] = taps[7:8]
    o_ra[...] = ra[...]
    o_rv[...] = rv[...]
    o_rd[...] = rd[...]
    o_cr[...] = jnp.concatenate([cr[:, 0:3], cr[:, 4:7]], axis=0)
    for copy in copies:
        copy.wait()


def per_device(sizes, hid, upa, upv, cot, wa, wv, wd, ca, cv, ba, bv):
    nz, ny, nx, nc = sizes
    n = nx * nc
    rows, hidden = upa.shape
    width = wd.shape[1]
    tokens = hid.shape[0]
    vm = pl.BlockSpec(memory_space=pltpu.VMEM)
    hbm = pl.BlockSpec(memory_space=pltpu.HBM)
    dma = pltpu.SemaphoreType.DMA

    def f32(*shape):
        return jax.ShapeDtypeStruct(shape, F32)

    outs = (
        jax.ShapeDtypeStruct((1, n * width), BF16),
        f32(hidden, width), f32(hidden, width), f32(hidden, width),
        f32(8, hidden), f32(1, width), f32(1, width), f32(1, hidden), f32(1, 128),
    )
    v = pltpu.VMEM
    scratch = [
        v((rows + 8, n * width), BF16), v((tokens, width), BF16), v((n, hidden, width), BF16),
        v((n, 2 * hidden, width), BF16), v((hidden, rows), BF16), v((hidden, rows), BF16),
        v(ca.shape, BF16), v(cv.shape, BF16), v(ba.shape, BF16), v(bv.shape, BF16),
        v((hidden, rows), BF16), v((hidden, rows), BF16), v((hidden, rows), BF16),
        v((n, 3 * hidden, rows), BF16), v((n, 8, hidden), F32), v((n, rows, width), BF16),
        v((rows, width), BF16), v((n, rows, width), F32),
        v((14, 4, nz, width), BF16), v((14, 4, nz, width), BF16),
        v((width // 128, rows, 128), F32), v((nz, n, width), BF16), v((nz, n, width), BF16),
        v((n, 1, width), F32),
        v((nz, 9, 1, 128), F32), v((ny, 9, 1, 128), F32), v((n, 1, hidden), F32),
        dma((11,)), dma((3,)), dma((3,)), dma((9,)), dma((9,)), dma((9,)), dma((9,)),
        dma((9,)), dma((9,)), dma((9,)), dma((9,)), dma((n,)), dma((n,)), dma((8,)), dma((8,)),
        dma((14,)), dma((14,)), dma((nz,)), dma((nz,)),
        dma((nz,)), dma((nz,)), dma((ny,)), dma((ny,)), dma((n,)), dma((n,)),
    ]
    res = pl.pallas_call(
        functools.partial(kernel, sizes),
        out_shape=outs,
        in_specs=[hbm] * 11,
        out_specs=[vm] * len(outs),
        scratch_shapes=scratch,
        compiler_params=pltpu.CompilerParams(
            collective_id=0, has_side_effects=True, vmem_limit_bytes=48 * 1024 * 1024
        ),
    )(*[pltpu.with_memory_space_constraint(v, pltpu.HBM) for v in (hid, upa.T, upv.T, cot, wa.T, wv.T, wd, ca, cv, ba, bv)])
    final = (
        jax.ShapeDtypeStruct((1, n * width), BF16),
        f32(hidden, width), f32(hidden, width), f32(hidden, width),
        f32(3, hidden), f32(3, hidden), f32(1, hidden), f32(1, hidden),
        f32(1, width), f32(1, width), f32(1, hidden), f32(2, 3),
    )
    gi, gwa, gwv, gwd, gca, gcv, gba, gbv, ra, rv, rd, conv_rows = pl.pallas_call(
        finish,
        out_shape=final,
        in_specs=[vm] * len(outs),
        out_specs=[vm, hbm, hbm, hbm] + [vm] * 8,
        scratch_shapes=[dma((3,))],
        compiler_params=pltpu.CompilerParams(vmem_limit_bytes=8 * 1024 * 1024),
    )(*res)
    return (
        gi, gwa.T, gwv.T, gwd, gca, gcv, gba[0], gbv[0], ra[0], rv[0], rd[0], conv_rows,
    )


def solution(mesh):
    sizes = (16, 8, 4, 2)
    finer = Mesh(mesh.devices.reshape(sizes), FS + TP)
    return jax.shard_map(
        functools.partial(per_device, sizes),
        mesh=finer,
        in_specs=(
            P(None, TP), P(TP, FS), P(TP, FS), P(TP, None), P(TP, FS), P(TP, FS),
            P(FS, TP), P(None, FS), P(None, FS), P(FS), P(FS),
        ),
        out_specs=(
            P(TP_FS, None), P(TP, FS), P(TP, FS), P(FS, TP), P(None, FS), P(None, FS),
            P(FS), P(FS), P(TP), P(TP), P(FS), P(),
        ),
        check_vma=False,
    )
```

```python
import functools

import jax
import jax.numpy as jnp
from jax import lax
from jax.experimental import pallas as pl
from jax.experimental.pallas import tpu as pltpu
from jax.sharding import Mesh
from jax.sharding import PartitionSpec as P

FS = ("fs_0", "fs_1")
TP = ("tp_0", "tp_1")
TP_FS = ("tp_0", "tp_1", "fs_0", "fs_1")
MESH = pl.DeviceIdType.MESH
F32 = jnp.float32
BF16 = jnp.bfloat16
ROOT_2_OVER_PI = 0.7978845608028654
CUBIC = 0.044715


def dot_nn(a, b):
    return lax.dot_general(a, b, (((1,), (0,)), ((), ())), preferred_element_type=F32)


def dot_nt(a, b):
    return lax.dot_general(a, b, (((1,), (1,)), ((), ())), preferred_element_type=F32)


def kernel(
    sizes,
    hid, upa, upv, cot, wa, wv, wd, ca, cv, ba, bv,
    o_gi, o_gwa, o_gwv, o_gwd, o_tap, o_ra, o_rv, o_rd, o_cr,
    cotx, hidv, wdall, wall, uas, uvs, cas, cvs, bas, bvs, hb, hprev, hnext,
    agb, tapb, cotc, relay, pbuf, ysend, yrecv, acc, zsend, zrecv, row_out,
    rz, ry, drecv,
    lsem, hs, hr, wds_, wdr, was, war, wvs, wvr, gs, gr, ts, tr, cs, cr,
    ys, yr, zs, zr, r1s, r1r, r2s, r2r, ds_, dr, tok,
):
    nz, ny, nx, nc = sizes
    z, y = lax.axis_index("fs_0"), lax.axis_index("fs_1")
    x, c = lax.axis_index("tp_0"), lax.axis_index("tp_1")
    j = x * 2 + c
    hidden, rows = upa.shape
    width = wd.shape[1]
    n = nx * nc
    pend = []

    def send(src, dst, ssem, rsem, device):
        copy = pltpu.make_async_remote_copy(
            src_ref=src, dst_ref=dst, send_sem=ssem, recv_sem=rsem,
            device_id=device, device_id_type=MESH,
        )
        copy.start()
        pend.append(copy)
        return copy

    barrier = pltpu.get_barrier_semaphore()

    def tp_device(k):
        other = lax.rem(j + k, n)
        return {"tp_0": other // nc, "tp_1": lax.rem(other, nc)}

    def both_sides(sem, axis, at, length, by):
        for k in (by, length - by):
            pl.semaphore_signal(
                sem, inc=1, device_id={axis: lax.rem(at + k, length)}, device_id_type=MESH
            )

    both_sides(barrier, "fs_0", z, nz, 1)
    both_sides(barrier, "fs_1", y, ny, 1)
    for k in range(1, n):
        pl.semaphore_signal(barrier, inc=1, device_id=tp_device(k), device_id_type=MESH)

    loads = []
    for i, (src, dst) in enumerate((
        (wd, wdall.at[j]), (upa, uas), (upv, uvs), (ca, cas), (cv, cvs), (ba, bas), (bv, bvs),
        (cot, cotx.at[pl.ds(0, rows)]), (wa, wall.at[j, pl.ds(0, hidden)]),
        (wv, wall.at[j, pl.ds(hidden, hidden)]), (hid, hidv),
    )):
        copy = pltpu.make_async_copy(src, dst, lsem.at[i])
        copy.start()
        loads.append(copy)
    for copy in loads[0:7]:
        copy.wait()

    lane = lax.broadcasted_iota(jnp.int32, (hidden, rows), 1)

    def roll(value, by):
        return pltpu.roll(value, by % rows, 1)

    ua, uv = uas[...].astype(F32), uvs[...].astype(F32)
    heads = jnp.where(lane < 2, ua, roll(uv, 2))
    tails = jnp.where(lane >= rows - 2, ua, roll(uv, -2))
    hb[...] = jnp.where(lane < rows // 2, heads, tails).astype(BF16)

    pl.semaphore_wait(barrier, n - 1 + 4)

    both_sides(tok.at[0], "fs_0", z, nz, 1)
    both_sides(tok.at[1], "fs_1", y, ny, 1)

    partner = {"tp_1": 1 - c}

    def chip(dx):
        return {"tp_0": lax.rem(x + dx, nx)}

    def slot_of(dx, core):
        return lax.rem(x + nx - dx, nx) * 2 + core

    slots = (
        j, x * 2 + 1 - c, slot_of(1, c), slot_of(3, c),
        slot_of(1, 1 - c), slot_of(3, 1 - c), slot_of(2, c), slot_of(2, 1 - c),
    )

    class Gather:
        def __init__(self, buf, first, count, ssem, rsem):
            self.buf, self.first, self.count, self.half = buf, first, count, count // 2
            self.ssem, self.rsem, self.copies = ssem, rsem, {}

        def go(self, i, slot, at, size, device):
            view = self.buf.at[slot, pl.ds(self.first + at, size)]
            self.copies[i] = send(view, view, self.ssem.at[i], self.rsem.at[i], device)

        def start(self):
            half = self.half
            self.go(1, j, 0, half, chip(1))
            self.go(2, j, half, half, chip(3))
            self.go(9, j, half, half, chip(1))
            self.go(10, j, 0, half, chip(3))
            self.go(0, j, 0, self.count, partner)

        def wait(self, *which):
            for i in which:
                self.copies[i].wait_recv()

        def pass_near(self):
            self.wait(1)
            self.go(3, slots[2], 0, self.half, chip(1))
            self.wait(2)
            self.go(4, slots[3], self.half, self.half, chip(3))
            self.wait(9)
            self.go(5, slots[2], 0, self.count, partner)
            self.wait(10)
            self.go(6, slots[3], 0, self.count, partner)

        def pass_far(self):
            self.wait(3)
            self.go(7, slots[6], 0, self.half, partner)
            self.wait(4)
            self.go(8, slots[6], self.half, self.half, partner)

    down_all = Gather(wdall, 0, hidden, wds_, wdr)
    act_all = Gather(wall, 0, hidden, was, war)
    val_all = Gather(wall, hidden, hidden, wvs, wvr)
    grads_all = Gather(agb, 0, 3 * hidden, gs, gr)
    down_all.start()
    up_dev, down_dev = tp_device(1), tp_device(n - 1)
    h_copy = [
        send(cot.at[pl.ds(0, 8)], cotx.at[pl.ds(rows, 8)], hs.at[0], hr.at[0], down_dev),
        send(hb, hnext, hs.at[1], hr.at[1], down_dev),
        send(hb, hprev, hs.at[2], hr.at[2], up_dev),
    ]

    for copy in loads[8:10]:
        copy.wait()
    act_all.start()

    out_row = lax.broadcasted_iota(jnp.int32, (rows, rows), 0)
    in_row = lax.broadcasted_iota(jnp.int32, (rows, rows), 1)
    order = (in_row == lax.rem(out_row, nz) * ny + out_row // nz).astype(F32).astype(BF16)
    table = jnp.concatenate(
        [cas[...].astype(F32), bas[...].astype(F32).reshape(1, hidden),
         cvs[...].astype(F32), bvs[...].astype(F32).reshape(1, hidden)], axis=0,
    ).T
    par_a = [table[:, k : k + 1] for k in range(4)]
    par_v = [table[:, k : k + 1] for k in range(4, 8)]

    down_all.pass_near()
    val_all.start()
    pl.semaphore_wait(tok.at[0], 2)
    pl.semaphore_wait(tok.at[1], 2)
    both_sides(tok.at[2], "fs_0", z, nz, 2)
    both_sides(tok.at[3], "fs_1", y, ny, 2)
    for copy in h_copy:
        copy.wait_recv()
    first = (j > 0).astype(F32)
    last = (j < n - 1).astype(F32)
    before = hprev[...].astype(F32) * first
    after = hnext[...].astype(F32)

    def ahead(par, u2, u1, u0):
        return par[3] + par[0] * u2 + par[1] * u1 + par[2] * u0

    def shifted(u, prev):
        u1 = jnp.where(lane < 1, roll(prev, 1), roll(u, 1))
        return jnp.where(lane < 2, roll(prev, 2), roll(u, 2)), u1, u

    def shifted_next(u, following):
        u1 = jnp.where(lane < 1, roll(u, 1), roll(following, 1))
        return [v[:, 0:8] for v in (roll(u, 2), u1, following)]

    ups_a = shifted(ua, before)
    ups_v = shifted(uv, roll(before, 2))
    next_a = shifted_next(ua, after)
    next_v = shifted_next(uv, roll(after, -2))

    def activation(pre_a, pre_v):
        square = pre_a * pre_a
        th = jnp.tanh(ROOT_2_OVER_PI * (pre_a + CUBIC * pre_a * square))
        half = 0.5 * (1.0 + th)
        gelu = pre_a * half
        slope = half + 0.5 * pre_a * (1.0 - th * th) * (ROOT_2_OVER_PI * (1.0 + 3.0 * CUBIC * square))
        return pre_v * slope, gelu, gelu * pre_v

    fac_a, fac_v, mixed = activation(ahead(par_a, *ups_a), ahead(par_v, *ups_v))
    nfac_a, nfac_v, _ = activation(ahead(par_a, *next_a), ahead(par_v, *next_v))
    agb[j, pl.ds(2 * hidden, hidden), :] = mixed.astype(BF16)

    loads[7].wait()

    def part(slot, block):
        return dot_nt(block, cotx[:, pl.ds(pl.multiple_of(slot * width, width), width)])

    gm = part(j, wdall[j])
    down_all.wait(0)
    gm = gm + part(slots[1], wdall[slots[1]])
    gm = gm + part(slots[2], wdall[slots[2]]) + part(slots[3], wdall[slots[3]])
    down_all.wait(5, 6)
    gm = gm + part(slots[4], wdall[slots[4]]) + part(slots[5], wdall[slots[5]])
    act_all.pass_near()
    down_all.pass_far()
    gm = gm + part(slots[6], wdall[slots[6]])
    pl.semaphore_wait(tok.at[2], 2)
    pl.semaphore_wait(tok.at[3], 2)
    both_sides(tok.at[4], "fs_0", z, nz, 4)
    down_all.wait(7, 8)
    gm = gm + part(slots[7], wdall[slots[7]])
    gm = gm.astype(BF16).astype(F32)
    gm_next = gm[:, rows:] * last
    gm = gm[:, 0:rows]
    grad_a, grad_v = gm * fac_a, gm * fac_v
    empty = jnp.zeros((hidden, rows - 8), F32)
    after_a = jnp.concatenate([gm_next * nfac_a, empty], axis=1)
    after_v = jnp.concatenate([gm_next * nfac_v, empty], axis=1)

    def behind(par, grad, following):
        g1 = jnp.where(lane < rows - 1, roll(grad, -1), roll(following, -1))
        g2 = jnp.where(lane < rows - 2, roll(grad, -2), roll(following, -2))
        return par[0] * g2 + par[1] * g1 + par[2] * grad

    agb[j, pl.ds(0, hidden), :] = behind(par_a, grad_a, after_a).astype(BF16)
    agb[j, pl.ds(hidden, hidden), :] = behind(par_v, grad_v, after_v).astype(BF16)
    val_all.pass_near()
    left = dot_nt(order, agb[j, pl.ds(0, 2 * hidden), :]).astype(BF16)

    def product(a):
        pbuf[a] = dot_nn(left, wall[slots[a]])

    def mine(k, half):
        at = pl.multiple_of(lax.rem(y + k + ny, ny) * nz, nz)
        return pbuf[pl.ds(4 * half, 4), pl.ds(at, nz), :]

    ring = {}

    def pass_on(i, value, step):
        ysend[i] = value.astype(BF16)
        ring[i] = send(
            ysend.at[i], yrecv.at[i], ys.at[i], yr.at[i], {"fs_1": lax.rem(y + step + ny, ny)}
        )

    def arrived(i):
        ring[i].wait_recv()
        return yrecv[i].astype(F32)

    product(0)
    act_all.wait(0)
    val_all.wait(0)
    product(1)
    product(2)
    product(3)
    pass_on(0, mine(4, 0), 1)
    pass_on(11, mine(-3, 0), -1)
    grads_all.start()

    act_all.wait(5, 6)
    val_all.wait(5, 6)
    product(4)
    product(5)
    act_all.pass_far()
    val_all.pass_far()
    product(6)
    act_all.wait(7, 8)
    val_all.wait(7, 8)
    product(7)
    pass_on(7, mine(-4, 1), -1)
    pass_on(4, mine(3, 1), 1)
    spread = jnp.zeros((hidden, rows), F32)
    at = 0
    for grad, ups in ((grad_a, ups_a), (grad_v, ups_v)):
        for k in range(4):
            terms = grad * ups[k] if k < 3 else grad
            spread = jnp.where(lane == at, jnp.sum(terms, axis=1, keepdims=True), spread)
            at += 1
    tapb[j] = spread.T[0:8]
    t_copy = [
        send(tapb.at[j], tapb.at[j], ts.at[k], tr.at[k], tp_device(k)) for k in range(1, n)
    ]

    grads_all.pass_near()
    pass_on(1, arrived(0) + mine(3, 0), 1)
    pass_on(12, arrived(11) + mine(-2, 0), -1)

    def columns(dx, core):
        at = (lax.rem(x + dx, nx) * 2 + core) * width
        return cotx.at[pl.ds(0, rows), pl.ds(pl.multiple_of(at, width), width)]

    c_copy = [
        send(columns(2, 1 - c), relay, cs.at[6], cr.at[6], {"tp_0": lax.rem(x + 3, nx), "tp_1": 1 - c})
    ]
    for i, (dx, core) in enumerate(((1, c), (3, c), (2, c), (1, 1 - c), (3, 1 - c), (0, 1 - c))):
        c_copy.append(
            send(
                columns(dx, core), cotc.at[j], cs.at[i], cr.at[i],
                {"tp_0": lax.rem(x + dx, nx), "tp_1": core},
            )
        )
    pass_on(8, arrived(7) + mine(-3, 1), -1)
    pass_on(5, arrived(4) + mine(2, 1), 1)
    pass_on(2, arrived(1) + mine(2, 0), 1)
    pass_on(13, arrived(12) + mine(-1, 0), -1)

    grads_all.wait(0, 5, 6)
    grads_all.pass_far()
    grads_all.wait(7, 8)
    loads[10].wait()
    gathered = jnp.concatenate([agb[s, pl.ds(0, 2 * hidden), :] for s in range(n)], axis=1)
    gwt = dot_nn(gathered, hidv[...])
    o_gwa[...] = gwt[0:hidden]
    o_gwv[...] = gwt[hidden:]
    squares = gwt * gwt
    row_a = jnp.sum(squares[0:hidden], axis=0, keepdims=True)
    row_v = jnp.sum(squares[hidden:], axis=0, keepdims=True)
    for copy in t_copy:
        copy.wait_recv()
    taps = tapb[0]
    for s in range(1, n):
        taps = taps + tapb[s]
    o_tap[...] = taps
    sums = jnp.sum(taps * taps, axis=1, keepdims=True)
    spot = lax.broadcasted_iota(jnp.int32, (8, 128), 0) == lax.broadcasted_iota(
        jnp.int32, (8, 128), 1
    )
    tiles = width // 128
    for k in range(tiles):
        rz[z, k] = row_a[:, 128 * k : 128 * (k + 1)]
        rz[z, tiles + k] = row_v[:, 128 * k : 128 * (k + 1)]
    pl.semaphore_wait(tok.at[4], 2)
    rz[z, 2 * tiles] = jnp.sum(jnp.where(spot, sums, 0.0), axis=0, keepdims=True)
    r1_copy = [
        send(rz.at[z], rz.at[z], r1s.at[k], r1r.at[k], {"fs_0": lax.rem(z + k, nz)})
        for k in range(1, nz)
    ]

    pass_on(9, arrived(8) + mine(-2, 1), -1)
    pass_on(6, arrived(5) + mine(1, 1), 1)
    pass_on(3, arrived(2) + mine(1, 0), 1)
    c_copy[0].wait_recv()
    c_copy.append(send(relay, cotc.at[slot_of(3, 1 - c)], cs.at[7], cr.at[7], chip(3)))
    pass_on(10, arrived(9) + mine(-1, 1), -1)
    z_copy = []
    for half, (i, k) in enumerate(((13, 3), (6, 10))):
        total = mine(0, half) + (arrived(i) + arrived(k))
        for b in range(4):
            for t in range(tiles):
                acc[half, t, pl.ds(b * nz, nz), :] = total[b, :, 128 * t : 128 * (t + 1)]
        for k in range(nz):
            for t in range(tiles):
                zsend[half, k, :, pl.ds(128 * t, 128)] = acc[
                    half, t, pl.ds(k, 4, stride=nz), :
                ].astype(BF16)
        for k in range(1, nz):
            other = lax.rem(z + k, nz)
            z_copy.append(
                send(
                    zsend.at[half, other], zrecv.at[half, z], zs.at[half, k], zr.at[half, k],
                    {"fs_0": other},
                )
            )
        zrecv[half, z] = zsend[half, z]

    for copy in r1_copy:
        copy.wait_recv()
    piece = rz[0]
    for s in range(1, nz):
        piece = piece + rz[s]
    ry[y] = piece
    r2_copy = [
        send(ry.at[y], ry.at[y], r2s.at[k], r2r.at[k], {"fs_1": lax.rem(y + k, ny)})
        for k in range(1, ny)
    ]

    for copy in c_copy[1:]:
        copy.wait_recv()
    cotc[j] = cotx[pl.ds(0, rows), pl.ds(pl.multiple_of(j * width, width), width)]
    mixed_all = jnp.concatenate([agb[s, pl.ds(2 * hidden, hidden), :] for s in range(n)], axis=1)
    gwd = dot_nn(mixed_all, cotc[...].reshape(n * rows, width))
    o_gwd[...] = gwd
    sq = gwd * gwd
    lanes = sq[:, 0:128]
    for k in range(1, tiles):
        lanes = lanes + sq[:, 128 * k : 128 * (k + 1)]
    drecv[j] = jnp.sum(lanes.T, axis=0, keepdims=True)
    d_copy = [
        send(drecv.at[j], drecv.at[j], ds_.at[k], dr.at[k], tp_device(k)) for k in range(1, n)
    ]

    for copy in r2_copy:
        copy.wait_recv()
    piece = ry[0]
    for s in range(1, ny):
        piece = piece + ry[s]
    for k in range(tiles):
        o_ra[:, pl.ds(128 * k, 128)] = piece[k]
        o_rv[:, pl.ds(128 * k, 128)] = piece[tiles + k]
    o_cr[...] = piece[2 * tiles]
    for copy in d_copy:
        copy.wait_recv()
    down = drecv[0]
    for s in range(1, n):
        down = down + drecv[s]
    o_rd[...] = down

    for copy in z_copy:
        copy.wait_recv()
    for half in range(2):
        total = zrecv[half, 0].astype(F32)
        for s in range(1, nz):
            total = total + zrecv[half, s].astype(F32)
        for a in range(4):
            row_out[slots[4 * half + a]] = total[a : a + 1]
    for s in range(n):
        o_gi[:, pl.ds(width * s, width)] = row_out[s].astype(BF16)
    for copy in pend:
        copy.wait_send()


def finish(gi, gwa, gwv, gwd, tap, ra, rv, rd, cr,
           o_gi, o_gwa, o_gwv, o_gwd, o_gca, o_gcv, o_gba, o_gbv, o_ra, o_rv, o_rd, o_cr,
           csem):
    copies = [
        pltpu.make_async_copy(src, dst, csem.at[i])
        for i, (src, dst) in enumerate(((gwa, o_gwa), (gwv, o_gwv), (gwd, o_gwd)))
    ]
    for copy in copies:
        copy.start()
    o_gi[...] = gi[...]
    taps = tap[...]
    o_gca[...] = taps[0:3]
    o_gba[...] = taps[3:4]
    o_gcv[...] = taps[4:7]
    o_gbv[...] = taps[7:8]
    o_ra[...] = ra[...]
    o_rv[...] = rv[...]
    o_rd[...] = rd[...]
    o_cr[...] = jnp.concatenate([cr[:, 0:3], cr[:, 4:7]], axis=0)
    for copy in copies:
        copy.wait()


def per_device(sizes, hid, upa, upv, cot, wa, wv, wd, ca, cv, ba, bv):
    nz, ny, nx, nc = sizes
    n = nx * nc
    rows, hidden = upa.shape
    width = wd.shape[1]
    tokens = hid.shape[0]
    vm = pl.BlockSpec(memory_space=pltpu.VMEM)
    hbm = pl.BlockSpec(memory_space=pltpu.HBM)
    dma = pltpu.SemaphoreType.DMA

    def f32(*shape):
        return jax.ShapeDtypeStruct(shape, F32)

    outs = (
        jax.ShapeDtypeStruct((1, n * width), BF16),
        f32(hidden, width), f32(hidden, width), f32(hidden, width),
        f32(8, hidden), f32(1, width), f32(1, width), f32(1, hidden), f32(1, 128),
    )
    v = pltpu.VMEM
    scratch = [
        v((rows + 8, n * width), BF16), v((tokens, width), BF16), v((n, hidden, width), BF16),
        v((n, 2 * hidden, width), BF16), v((hidden, rows), BF16), v((hidden, rows), BF16),
        v(ca.shape, BF16), v(cv.shape, BF16), v(ba.shape, BF16), v(bv.shape, BF16),
        v((hidden, rows), BF16), v((hidden, rows), BF16), v((hidden, rows), BF16),
        v((n, 3 * hidden, rows), BF16), v((n, 8, hidden), F32), v((n, rows, width), BF16),
        v((rows, width), BF16), v((n, rows, width), F32),
        v((14, 4, nz, width), BF16), v((14, 4, nz, width), BF16),
        v((2, width // 128, 4 * nz, 128), F32),
        v((2, nz, 4, width), BF16), v((2, nz, 4, width), BF16),
        v((n, 1, width), F32),
        v((nz, 9, 1, 128), F32), v((ny, 9, 1, 128), F32), v((n, 1, hidden), F32),
        dma((11,)), dma((3,)), dma((3,)), dma((11,)), dma((11,)), dma((11,)), dma((11,)),
        dma((11,)), dma((11,)), dma((11,)), dma((11,)), dma((n,)), dma((n,)), dma((8,)), dma((8,)),
        dma((14,)), dma((14,)), dma((2, nz)), dma((2, nz)),
        dma((nz,)), dma((nz,)), dma((ny,)), dma((ny,)), dma((n,)), dma((n,)),
        pltpu.SemaphoreType.REGULAR((5,)),
    ]
    res = pl.pallas_call(
        functools.partial(kernel, sizes),
        out_shape=outs,
        in_specs=[hbm] * 11,
        out_specs=[vm] * len(outs),
        scratch_shapes=scratch,
        compiler_params=pltpu.CompilerParams(
            collective_id=0, has_side_effects=True, vmem_limit_bytes=48 * 1024 * 1024
        ),
    )(*[pltpu.with_memory_space_constraint(v, pltpu.HBM) for v in (hid, upa.T, upv.T, cot, wa.T, wv.T, wd, ca, cv, ba, bv)])
    final = (
        jax.ShapeDtypeStruct((1, n * width), BF16),
        f32(hidden, width), f32(hidden, width), f32(hidden, width),
        f32(3, hidden), f32(3, hidden), f32(1, hidden), f32(1, hidden),
        f32(1, width), f32(1, width), f32(1, hidden), f32(2, 3),
    )
    gi, gwa, gwv, gwd, gca, gcv, gba, gbv, ra, rv, rd, conv_rows = pl.pallas_call(
        finish,
        out_shape=final,
        in_specs=[vm] * len(outs),
        out_specs=[vm, hbm, hbm, hbm] + [vm] * 8,
        scratch_shapes=[dma((3,))],
        compiler_params=pltpu.CompilerParams(vmem_limit_bytes=8 * 1024 * 1024),
    )(*res)
    return (
        gi, gwa.T, gwv.T, gwd, gca, gcv, gba[0], gbv[0], ra[0], rv[0], rd[0], conv_rows,
    )


def solution(mesh):
    sizes = (16, 8, 4, 2)
    finer = Mesh(mesh.devices.reshape(sizes), FS + TP)
    return jax.shard_map(
        functools.partial(per_device, sizes),
        mesh=finer,
        in_specs=(
            P(None, TP), P(TP, FS), P(TP, FS), P(TP, None), P(TP, FS), P(TP, FS),
            P(FS, TP), P(None, FS), P(None, FS), P(FS), P(FS),
        ),
        out_specs=(
            P(TP_FS, None), P(TP, FS), P(TP, FS), P(FS, TP), P(None, FS), P(None, FS),
            P(FS), P(FS), P(TP), P(TP), P(FS), P(),
        ),
        check_vma=False,
    )
```

```python
import functools

import jax
import jax.numpy as jnp
from jax import lax
from jax.experimental import pallas as pl
from jax.experimental.pallas import tpu as pltpu
from jax.sharding import Mesh
from jax.sharding import PartitionSpec as P

FS = ("fs_0", "fs_1")
TP = ("tp_0", "tp_1")
TP_FS = ("tp_0", "tp_1", "fs_0", "fs_1")
MESH = pl.DeviceIdType.MESH
F32 = jnp.float32
BF16 = jnp.bfloat16
ROOT_2_OVER_PI = 0.7978845608028654
CUBIC = 0.044715


def dot_nn(a, b):
    return lax.dot_general(a, b, (((1,), (0,)), ((), ())), preferred_element_type=F32)


def dot_nt(a, b):
    return lax.dot_general(a, b, (((1,), (1,)), ((), ())), preferred_element_type=F32)


def kernel(
    sizes,
    hid, upa, upv, cot, wa, wv, wd, ca, cv, ba, bv,
    o_gi, o_gwa, o_gwv, o_gwd, o_tap, o_ra, o_rv, o_rd, o_cr,
    cotx, hidv, wdall, wall, uas, uvs, cas, cvs, bas, bvs, hb, hprev, hnext,
    agb, tapb, cotc, relay, pbuf, ysend, yrecv, acc, zsend, zrecv, row_out,
    rz, ry, drecv,
    lsem, hs, hr, wds_, wdr, was, war, wvs, wvr, gs, gr, ts, tr, cs, cr,
    ys, yr, zs, zr, r1s, r1r, r2s, r2r, ds_, dr, tok,
):
    nz, ny, nx, nc = sizes
    z, y = lax.axis_index("fs_0"), lax.axis_index("fs_1")
    x, c = lax.axis_index("tp_0"), lax.axis_index("tp_1")
    j = x * 2 + c
    hidden, rows = upa.shape
    width = wd.shape[1]
    n = nx * nc
    pend = []

    def send(src, dst, ssem, rsem, device):
        copy = pltpu.make_async_remote_copy(
            src_ref=src, dst_ref=dst, send_sem=ssem, recv_sem=rsem,
            device_id=device, device_id_type=MESH,
        )
        copy.start()
        pend.append(copy)
        return copy

    barrier = pltpu.get_barrier_semaphore()

    def tp_device(k):
        other = lax.rem(j + k, n)
        return {"tp_0": other // nc, "tp_1": lax.rem(other, nc)}

    def both_sides(sem, axis, at, length, by):
        for k in (by, length - by):
            pl.semaphore_signal(
                sem, inc=1, device_id={axis: lax.rem(at + k, length)}, device_id_type=MESH
            )

    both_sides(barrier, "fs_0", z, nz, 1)
    both_sides(barrier, "fs_1", y, ny, 1)
    for k in range(1, n):
        pl.semaphore_signal(barrier, inc=1, device_id=tp_device(k), device_id_type=MESH)

    loads = []
    for i, (src, dst) in enumerate((
        (wd, wdall.at[j]), (upa, uas), (upv, uvs), (ca, cas), (cv, cvs), (ba, bas), (bv, bvs),
        (cot, cotx.at[pl.ds(0, rows)]), (wa, wall.at[j, pl.ds(0, hidden)]),
        (wv, wall.at[j, pl.ds(hidden, hidden)]), (hid, hidv),
    )):
        copy = pltpu.make_async_copy(src, dst, lsem.at[i])
        copy.start()
        loads.append(copy)
    for copy in loads[0:7]:
        copy.wait()

    lane = lax.broadcasted_iota(jnp.int32, (hidden, rows), 1)

    def roll(value, by):
        return pltpu.roll(value, by % rows, 1)

    ua, uv = uas[...].astype(F32), uvs[...].astype(F32)
    heads = jnp.where(lane < 2, ua, roll(uv, 2))
    tails = jnp.where(lane >= rows - 2, ua, roll(uv, -2))
    hb[...] = jnp.where(lane < rows // 2, heads, tails).astype(BF16)

    pl.semaphore_wait(barrier, n - 1 + 4)

    both_sides(tok.at[0], "fs_0", z, nz, 1)
    both_sides(tok.at[1], "fs_1", y, ny, 1)

    partner = {"tp_1": 1 - c}

    def chip(dx):
        return {"tp_0": lax.rem(x + dx, nx)}

    def slot_of(dx, core):
        return lax.rem(x + nx - dx, nx) * 2 + core

    slots = (
        j, x * 2 + 1 - c, slot_of(1, c), slot_of(3, c),
        slot_of(1, 1 - c), slot_of(3, 1 - c), slot_of(2, c), slot_of(2, 1 - c),
    )

    class Gather:
        def __init__(self, buf, first, count, ssem, rsem):
            self.buf, self.first, self.count, self.half = buf, first, count, count // 2
            self.ssem, self.rsem, self.copies = ssem, rsem, {}

        def go(self, i, slot, at, size, device):
            view = self.buf.at[slot, pl.ds(self.first + at, size)]
            self.copies[i] = send(view, view, self.ssem.at[i], self.rsem.at[i], device)

        def start(self):
            half = self.half
            self.go(1, j, 0, half, chip(1))
            self.go(2, j, half, half, chip(3))
            self.go(9, j, half, half, chip(1))
            self.go(10, j, 0, half, chip(3))
            self.go(0, j, 0, self.count, partner)

        def wait(self, *which):
            for i in which:
                self.copies[i].wait_recv()

        def pass_near(self):
            self.wait(1)
            self.go(3, slots[2], 0, self.half, chip(1))
            self.wait(2)
            self.go(4, slots[3], self.half, self.half, chip(3))
            self.wait(9)
            self.go(5, slots[2], 0, self.count, partner)
            self.wait(10)
            self.go(6, slots[3], 0, self.count, partner)

        def pass_far(self):
            self.wait(3)
            self.go(7, slots[6], 0, self.half, partner)
            self.wait(4)
            self.go(8, slots[6], self.half, self.half, partner)

    down_all = Gather(wdall, 0, hidden, wds_, wdr)
    act_all = Gather(wall, 0, hidden, was, war)
    val_all = Gather(wall, hidden, hidden, wvs, wvr)
    grads_all = Gather(agb, 0, 3 * hidden, gs, gr)
    down_all.start()
    up_dev, down_dev = tp_device(1), tp_device(n - 1)
    h_copy = [
        send(cot.at[pl.ds(0, 8)], cotx.at[pl.ds(rows, 8)], hs.at[0], hr.at[0], down_dev),
        send(hb, hnext, hs.at[1], hr.at[1], down_dev),
        send(hb, hprev, hs.at[2], hr.at[2], up_dev),
    ]

    for copy in loads[8:10]:
        copy.wait()
    act_all.start()

    out_row = lax.broadcasted_iota(jnp.int32, (rows, rows), 0)
    in_row = lax.broadcasted_iota(jnp.int32, (rows, rows), 1)
    order = (in_row == lax.rem(out_row, nz) * ny + out_row // nz).astype(F32).astype(BF16)
    table = jnp.concatenate(
        [cas[...].astype(F32), bas[...].astype(F32).reshape(1, hidden),
         cvs[...].astype(F32), bvs[...].astype(F32).reshape(1, hidden)], axis=0,
    ).T
    par_a = [table[:, k : k + 1] for k in range(4)]
    par_v = [table[:, k : k + 1] for k in range(4, 8)]

    down_all.pass_near()
    val_all.start()
    pl.semaphore_wait(tok.at[0], 2)
    pl.semaphore_wait(tok.at[1], 2)
    both_sides(tok.at[2], "fs_0", z, nz, 2)
    both_sides(tok.at[3], "fs_1", y, ny, 2)
    for copy in h_copy:
        copy.wait_recv()
    first = (j > 0).astype(F32)
    last = (j < n - 1).astype(F32)
    before = hprev[...].astype(F32) * first
    after = hnext[...].astype(F32)

    def ahead(par, u2, u1, u0):
        return par[3] + par[0] * u2 + par[1] * u1 + par[2] * u0

    def shifted(u, prev):
        u1 = jnp.where(lane < 1, roll(prev, 1), roll(u, 1))
        return jnp.where(lane < 2, roll(prev, 2), roll(u, 2)), u1, u

    def shifted_next(u, following):
        u1 = jnp.where(lane < 1, roll(u, 1), roll(following, 1))
        return [v[:, 0:8] for v in (roll(u, 2), u1, following)]

    ups_a = shifted(ua, before)
    ups_v = shifted(uv, roll(before, 2))
    next_a = shifted_next(ua, after)
    next_v = shifted_next(uv, roll(after, -2))

    def activation(pre_a, pre_v):
        square = pre_a * pre_a
        th = jnp.tanh(ROOT_2_OVER_PI * (pre_a + CUBIC * pre_a * square))
        half = 0.5 * (1.0 + th)
        gelu = pre_a * half
        slope = half + 0.5 * pre_a * (1.0 - th * th) * (ROOT_2_OVER_PI * (1.0 + 3.0 * CUBIC * square))
        return pre_v * slope, gelu, gelu * pre_v

    fac_a, fac_v, mixed = activation(ahead(par_a, *ups_a), ahead(par_v, *ups_v))
    nfac_a, nfac_v, _ = activation(ahead(par_a, *next_a), ahead(par_v, *next_v))
    agb[j, pl.ds(2 * hidden, hidden), :] = mixed.astype(BF16)

    loads[7].wait()

    def part(slot, block):
        return dot_nt(block, cotx[:, pl.ds(pl.multiple_of(slot * width, width), width)])

    gm = part(j, wdall[j])
    down_all.wait(0)
    gm = gm + part(slots[1], wdall[slots[1]])
    gm = gm + part(slots[2], wdall[slots[2]]) + part(slots[3], wdall[slots[3]])
    down_all.wait(5, 6)
    gm = gm + part(slots[4], wdall[slots[4]]) + part(slots[5], wdall[slots[5]])
    act_all.pass_near()
    down_all.pass_far()
    gm = gm + part(slots[6], wdall[slots[6]])
    pl.semaphore_wait(tok.at[2], 2)
    pl.semaphore_wait(tok.at[3], 2)
    both_sides(tok.at[4], "fs_0", z, nz, 4)
    down_all.wait(7, 8)
    gm = gm + part(slots[7], wdall[slots[7]])
    gm = gm.astype(BF16).astype(F32)
    gm_next = gm[:, rows:] * last
    gm = gm[:, 0:rows]
    grad_a, grad_v = gm * fac_a, gm * fac_v
    empty = jnp.zeros((hidden, rows - 8), F32)
    after_a = jnp.concatenate([gm_next * nfac_a, empty], axis=1)
    after_v = jnp.concatenate([gm_next * nfac_v, empty], axis=1)

    def behind(par, grad, following):
        g1 = jnp.where(lane < rows - 1, roll(grad, -1), roll(following, -1))
        g2 = jnp.where(lane < rows - 2, roll(grad, -2), roll(following, -2))
        return par[0] * g2 + par[1] * g1 + par[2] * grad

    agb[j, pl.ds(0, hidden), :] = behind(par_a, grad_a, after_a).astype(BF16)
    agb[j, pl.ds(hidden, hidden), :] = behind(par_v, grad_v, after_v).astype(BF16)
    val_all.pass_near()
    left = dot_nt(order, agb[j, pl.ds(0, 2 * hidden), :]).astype(BF16)

    def product(a):
        pbuf[a] = dot_nn(left, wall[slots[a]])

    def mine(k, half):
        at = pl.multiple_of(lax.rem(y + k + ny, ny) * nz, nz)
        return pbuf[pl.ds(4 * half, 4), pl.ds(at, nz), :]

    ring = {}

    def pass_on(i, value, step):
        ysend[i] = value.astype(BF16)
        ring[i] = send(
            ysend.at[i], yrecv.at[i], ys.at[i], yr.at[i], {"fs_1": lax.rem(y + step + ny, ny)}
        )

    def arrived(i):
        ring[i].wait_recv()
        return yrecv[i].astype(F32)

    product(0)
    act_all.wait(0)
    val_all.wait(0)
    product(1)
    product(2)
    product(3)
    pass_on(0, mine(4, 0), 1)
    pass_on(11, mine(-3, 0), -1)
    grads_all.start()

    act_all.wait(5, 6)
    val_all.wait(5, 6)
    product(4)
    product(5)
    act_all.pass_far()
    val_all.pass_far()
    product(6)
    act_all.wait(7, 8)
    val_all.wait(7, 8)
    product(7)
    pass_on(7, mine(-4, 1), -1)
    pass_on(4, mine(3, 1), 1)
    spread = jnp.zeros((hidden, rows), F32)
    at = 0
    for grad, ups in ((grad_a, ups_a), (grad_v, ups_v)):
        for k in range(4):
            terms = grad * ups[k] if k < 3 else grad
            spread = jnp.where(lane == at, jnp.sum(terms, axis=1, keepdims=True), spread)
            at += 1
    tapb[j] = spread.T[0:8]
    t_copy = [
        send(tapb.at[j], tapb.at[j], ts.at[k], tr.at[k], tp_device(k)) for k in range(1, n)
    ]

    grads_all.pass_near()
    pass_on(1, arrived(0) + mine(3, 0), 1)
    pass_on(12, arrived(11) + mine(-2, 0), -1)

    def columns(dx, core):
        at = (lax.rem(x + dx, nx) * 2 + core) * width
        return cotx.at[pl.ds(0, rows), pl.ds(pl.multiple_of(at, width), width)]

    c_copy = [
        send(columns(2, 1 - c), relay, cs.at[6], cr.at[6], {"tp_0": lax.rem(x + 3, nx), "tp_1": 1 - c})
    ]
    for i, (dx, core) in enumerate(((1, c), (3, c), (2, c), (1, 1 - c), (3, 1 - c), (0, 1 - c))):
        c_copy.append(
            send(
                columns(dx, core), cotc.at[j], cs.at[i], cr.at[i],
                {"tp_0": lax.rem(x + dx, nx), "tp_1": core},
            )
        )
    pass_on(8, arrived(7) + mine(-3, 1), -1)
    pass_on(5, arrived(4) + mine(2, 1), 1)
    pass_on(2, arrived(1) + mine(2, 0), 1)
    pass_on(13, arrived(12) + mine(-1, 0), -1)

    grads_all.wait(0, 5, 6)
    grads_all.pass_far()
    grads_all.wait(7, 8)
    loads[10].wait()
    gathered = jnp.concatenate([agb[s, pl.ds(0, 2 * hidden), :] for s in range(n)], axis=1)
    gwt = dot_nn(gathered, hidv[...])
    o_gwa[...] = gwt[0:hidden]
    o_gwv[...] = gwt[hidden:]
    squares = gwt * gwt
    row_a = jnp.sum(squares[0:hidden], axis=0, keepdims=True)
    row_v = jnp.sum(squares[hidden:], axis=0, keepdims=True)
    for copy in t_copy:
        copy.wait_recv()
    taps = tapb[0]
    for s in range(1, n):
        taps = taps + tapb[s]
    o_tap[...] = taps
    sums = jnp.sum(taps * taps, axis=1, keepdims=True)
    spot = lax.broadcasted_iota(jnp.int32, (8, 128), 0) == lax.broadcasted_iota(
        jnp.int32, (8, 128), 1
    )
    tiles = width // 128
    for k in range(tiles):
        rz[z, k] = row_a[:, 128 * k : 128 * (k + 1)]
        rz[z, tiles + k] = row_v[:, 128 * k : 128 * (k + 1)]
    pl.semaphore_wait(tok.at[4], 2)
    rz[z, 2 * tiles] = jnp.sum(jnp.where(spot, sums, 0.0), axis=0, keepdims=True)
    r1_copy = [
        send(rz.at[z], rz.at[z], r1s.at[k], r1r.at[k], {"fs_0": lax.rem(z + k, nz)})
        for k in range(1, nz)
    ]

    pass_on(9, arrived(8) + mine(-2, 1), -1)
    pass_on(6, arrived(5) + mine(1, 1), 1)
    pass_on(3, arrived(2) + mine(1, 0), 1)
    c_copy[0].wait_recv()
    c_copy.append(send(relay, cotc.at[slot_of(3, 1 - c)], cs.at[7], cr.at[7], chip(3)))
    pass_on(10, arrived(9) + mine(-1, 1), -1)
    z_copy = []
    for half, (i, k) in enumerate(((13, 3), (6, 10))):
        total = mine(0, half) + (arrived(i) + arrived(k))
        for b in range(4):
            for t in range(tiles):
                acc[half, t, pl.ds(b * nz, nz), :] = total[b, :, 128 * t : 128 * (t + 1)]
        for k in range(nz):
            for t in range(tiles):
                zsend[half, k, :, pl.ds(128 * t, 128)] = acc[
                    half, t, pl.ds(k, 4, stride=nz), :
                ].astype(BF16)
        for k in range(1, nz):
            other = lax.rem(z + k, nz)
            z_copy.append(
                send(
                    zsend.at[half, other], zrecv.at[half, z], zs.at[half, k], zr.at[half, k],
                    {"fs_0": other},
                )
            )
        zrecv[half, z] = zsend[half, z]

    for copy in r1_copy:
        copy.wait_recv()
    piece = rz[0]
    for s in range(1, nz):
        piece = piece + rz[s]
    ry[y] = piece
    r2_copy = [
        send(ry.at[y], ry.at[y], r2s.at[k], r2r.at[k], {"fs_1": lax.rem(y + k, ny)})
        for k in range(1, ny)
    ]

    for copy in c_copy[1:]:
        copy.wait_recv()
    cotc[j] = cotx[pl.ds(0, rows), pl.ds(pl.multiple_of(j * width, width), width)]
    mixed_all = jnp.concatenate([agb[s, pl.ds(2 * hidden, hidden), :] for s in range(n)], axis=1)
    gwd = dot_nn(mixed_all, cotc[...].reshape(n * rows, width))
    o_gwd[...] = gwd
    sq = gwd * gwd
    lanes = sq[:, 0:128]
    for k in range(1, tiles):
        lanes = lanes + sq[:, 128 * k : 128 * (k + 1)]
    drecv[j] = jnp.sum(lanes.T, axis=0, keepdims=True)
    d_copy = [
        send(drecv.at[j], drecv.at[j], ds_.at[k], dr.at[k], tp_device(k)) for k in range(1, n)
    ]

    for copy in r2_copy:
        copy.wait_recv()
    piece = ry[0]
    for s in range(1, ny):
        piece = piece + ry[s]
    for k in range(tiles):
        o_ra[:, pl.ds(128 * k, 128)] = piece[k]
        o_rv[:, pl.ds(128 * k, 128)] = piece[tiles + k]
    o_cr[...] = piece[2 * tiles]
    for copy in d_copy:
        copy.wait_recv()
    down = drecv[0]
    for s in range(1, n):
        down = down + drecv[s]
    o_rd[...] = down

    for copy in pend:
        copy.wait_send()
    for half in range(2):
        for copy in z_copy[half * (nz - 1) : (half + 1) * (nz - 1)]:
            copy.wait_recv()
        total = zrecv[half, 0].astype(F32)
        for s in range(1, nz):
            total = total + zrecv[half, s].astype(F32)
        for a in range(4):
            row_out[slots[4 * half + a]] = total[a : a + 1]
    for s in range(n):
        o_gi[:, pl.ds(width * s, width)] = row_out[s].astype(BF16)


def finish(gi, gwa, gwv, gwd, tap, ra, rv, rd, cr,
           o_gi, o_gwa, o_gwv, o_gwd, o_gca, o_gcv, o_gba, o_gbv, o_ra, o_rv, o_rd, o_cr,
           t_gca, t_gcv, t_gba, t_gbv, t_cr, csem):
    taps = tap[...]
    t_gca[...] = taps[0:3]
    t_gba[...] = taps[3:4]
    t_gcv[...] = taps[4:7]
    t_gbv[...] = taps[7:8]
    t_cr[...] = jnp.concatenate([cr[:, 0:3], cr[:, 4:7]], axis=0)
    copies = [
        pltpu.make_async_copy(src, dst, csem.at[i])
        for i, (src, dst) in enumerate((
            (gwa, o_gwa), (gwv, o_gwv), (gwd, o_gwd), (gi, o_gi), (ra, o_ra), (rv, o_rv), (rd, o_rd),
            (t_gca, o_gca), (t_gcv, o_gcv), (t_gba, o_gba), (t_gbv, o_gbv), (t_cr, o_cr),
        ))
    ]
    for copy in copies:
        copy.start()
    for copy in copies:
        copy.wait()


def per_device(sizes, hid, upa, upv, cot, wa, wv, wd, ca, cv, ba, bv):
    nz, ny, nx, nc = sizes
    n = nx * nc
    rows, hidden = upa.shape
    width = wd.shape[1]
    tokens = hid.shape[0]
    vm = pl.BlockSpec(memory_space=pltpu.VMEM)
    hbm = pl.BlockSpec(memory_space=pltpu.HBM)
    dma = pltpu.SemaphoreType.DMA

    def f32(*shape):
        return jax.ShapeDtypeStruct(shape, F32)

    outs = (
        jax.ShapeDtypeStruct((1, n * width), BF16),
        f32(hidden, width), f32(hidden, width), f32(hidden, width),
        f32(8, hidden), f32(1, width), f32(1, width), f32(1, hidden), f32(1, 128),
    )
    v = pltpu.VMEM
    scratch = [
        v((rows + 8, n * width), BF16), v((tokens, width), BF16), v((n, hidden, width), BF16),
        v((n, 2 * hidden, width), BF16), v((hidden, rows), BF16), v((hidden, rows), BF16),
        v(ca.shape, BF16), v(cv.shape, BF16), v(ba.shape, BF16), v(bv.shape, BF16),
        v((hidden, rows), BF16), v((hidden, rows), BF16), v((hidden, rows), BF16),
        v((n, 3 * hidden, rows), BF16), v((n, 8, hidden), F32), v((n, rows, width), BF16),
        v((rows, width), BF16), v((n, rows, width), F32),
        v((14, 4, nz, width), BF16), v((14, 4, nz, width), BF16),
        v((2, width // 128, 4 * nz, 128), F32),
        v((2, nz, 4, width), BF16), v((2, nz, 4, width), BF16),
        v((n, 1, width), F32),
        v((nz, 9, 1, 128), F32), v((ny, 9, 1, 128), F32), v((n, 1, hidden), F32),
        dma((11,)), dma((3,)), dma((3,)), dma((11,)), dma((11,)), dma((11,)), dma((11,)),
        dma((11,)), dma((11,)), dma((11,)), dma((11,)), dma((n,)), dma((n,)), dma((8,)), dma((8,)),
        dma((14,)), dma((14,)), dma((2, nz)), dma((2, nz)),
        dma((nz,)), dma((nz,)), dma((ny,)), dma((ny,)), dma((n,)), dma((n,)),
        pltpu.SemaphoreType.REGULAR((5,)),
    ]
    res = pl.pallas_call(
        functools.partial(kernel, sizes),
        out_shape=outs,
        in_specs=[hbm] * 11,
        out_specs=[vm] * len(outs),
        scratch_shapes=scratch,
        compiler_params=pltpu.CompilerParams(
            collective_id=0, has_side_effects=True, vmem_limit_bytes=48 * 1024 * 1024
        ),
    )(*[pltpu.with_memory_space_constraint(v, pltpu.HBM) for v in (hid, upa.T, upv.T, cot, wa.T, wv.T, wd, ca, cv, ba, bv)])
    final = (
        jax.ShapeDtypeStruct((1, n * width), BF16),
        f32(hidden, width), f32(hidden, width), f32(hidden, width),
        f32(3, hidden), f32(3, hidden), f32(1, hidden), f32(1, hidden),
        f32(1, width), f32(1, width), f32(1, hidden), f32(2, 3),
    )
    gi, gwa, gwv, gwd, gca, gcv, gba, gbv, ra, rv, rd, conv_rows = pl.pallas_call(
        finish,
        out_shape=final,
        in_specs=[vm] * len(outs),
        out_specs=[hbm] * 12,
        scratch_shapes=[v(o.shape, F32) for o in (final[4], final[5], final[6], final[7], final[11])] + [dma((12,))],
        compiler_params=pltpu.CompilerParams(vmem_limit_bytes=8 * 1024 * 1024),
    )(*res)
    return (
        gi, gwa.T, gwv.T, gwd, gca, gcv, gba[0], gbv[0], ra[0], rv[0], rd[0], conv_rows,
    )


def solution(mesh):
    sizes = (16, 8, 4, 2)
    finer = Mesh(mesh.devices.reshape(sizes), FS + TP)
    return jax.shard_map(
        functools.partial(per_device, sizes),
        mesh=finer,
        in_specs=(
            P(None, TP), P(TP, FS), P(TP, FS), P(TP, None), P(TP, FS), P(TP, FS),
            P(FS, TP), P(None, FS), P(None, FS), P(FS), P(FS),
        ),
        out_specs=(
            P(TP_FS, None), P(TP, FS), P(TP, FS), P(FS, TP), P(None, FS), P(None, FS),
            P(FS), P(FS), P(TP), P(TP), P(FS), P(),
        ),
        check_vma=False,
    )
```
